32 devices in a mesh: sp: 16 (over z, y, x), tp: 2 (over core).
Axes of the slice: x: 2, y: 2, z: 4, core: 2. Of those that a mesh axis runs over, the one named last changes fastest.
Arguments:
- value_in: bfloat16 [5760, 2048], P('sp', 'tp'), may hold values from -240 to 240
- gate_in: bfloat16 [5760, 2048], P('sp', 'tp'), may hold values from -8 to 8
- taps: float32 [31, 2048], P(None, 'tp'), may hold values from -1 to 1
- norm_gain: float32 [2048], P('tp'), may hold values from 0.1 to 1.9
- norm_bias: float32 [2048], P('tp'), may hold values from -3 to 3
- proj_weight: bfloat16 [2048, 4096], P('tp', 'sp'), may hold values from -0.125 to 0.125
- out_grad: bfloat16 [5760, 4096], P('sp'), may hold values from -6 to 6
Outputs:
- value_grad: bfloat16 [5760, 2048], P('sp', 'tp')
- gate_grad: bfloat16 [5760, 2048], P('sp', 'tp')
- tap_grad: float32 [31, 2048], P(None, 'tp')
- gain_grad: float32 [2048], P('tp')
- bias_grad: float32 [2048], P('tp')
- weight_grad: float32 [2048, 4096], P('tp', 'sp')
The draws below stay inside these ranges and needn't reach their ends.
All inputs are finite; a program needn't handle non-finite values.
Results may differ from the reference program's by a relative error of at most 0.0051.
Values may be sent and summed in bfloat16 or wider, within the bound.
A program may use at most 64 MiB of HBM per device.

```python
import math
import jax
import jax.numpy as jnp
from jax import lax

MODEL = 4096
CHANNELS = 2048
TAPS = 31
TOKENS = 5760


def draw_value_in(key, part):
    first, second = jax.random.split(key, 2)
    chan = jnp.exp(jnp.linspace(0.0, math.log(10.0), CHANNELS)) * jax.random.uniform(second, (CHANNELS,), jnp.float32, 0.5, 2.0)
    along = jnp.exp(jnp.linspace(0.0, math.log(3.0), TOKENS))[:, None]
    base = jnp.clip(jax.random.normal(first, (TOKENS, CHANNELS), jnp.float32), -4.0, 4.0)
    return jnp.clip(base * chan[None, :] * along, -240.0, 240.0).astype(jnp.bfloat16)


def with_spikes(drawn, rng, source, target, blocks, factor):
    def block_of(position):
        return (jnp.arange(drawn.shape[position]) // (drawn.shape[position] // blocks)).reshape((-1,) + (1,) * (drawn.ndim - 1 - position))

    one_side = jax.random.permutation(rng, blocks)[block_of(target)]
    second = (block_of(target) + blocks // 2) % blocks
    return jnp.where((block_of(source) == one_side) | (block_of(source) == second), factor * drawn, drawn)


def levels(rng, shape, cuts, smallest, largest):
    loudness = 1.0
    for axis_at, shards_of in cuts:
        heights = jax.random.uniform(jax.random.fold_in(jax.random.fold_in(rng, 6), axis_at), (shards_of,), jnp.float32, smallest / len(cuts), largest / len(cuts))
        loudness = loudness * jnp.repeat(jnp.exp(heights), shape[axis_at] // shards_of).reshape((-1,) + (1,) * (len(shape) - 1 - axis_at))
    return loudness


def gaussian(key, dims, width, most, cuts=(), dtype=jnp.bfloat16):
    loudness = levels(key, dims, cuts, -0.22, 0.18) if cuts else 1.0
    values = jax.random.normal(key, dims, jnp.float32) * width * loudness
    return jnp.minimum(jnp.maximum(values, -most), most).astype(dtype)


def heavy_noise(stream_key, shape, scale, reach, cuts, heavy, kind=jnp.bfloat16):
    values = scale * jax.random.normal(stream_key, shape, jnp.float32)
    if cuts:
        values = values * levels(stream_key, shape, cuts, -0.22, 0.18)
    return jnp.clip(with_spikes(values, jax.random.fold_in(stream_key, 3), *heavy), -reach, reach).astype(kind)


def setup_inputs(seed: int = 0) -> dict:
    streams_of = jax.random.split(jax.random.key(seed), 8)
    return {
        "value_in": draw_value_in(jax.random.fold_in(streams_of[7], 71), 0),
        "gate_in": gaussian(streams_of[1], (TOKENS, CHANNELS), 2.0, 8.0, ((0, 16), (1, 2))),
        "taps": gaussian(streams_of[2], (TAPS, CHANNELS), TAPS ** -0.5, 1.0, ((1, 2),), jnp.float32),
        "norm_gain": jnp.clip(1.0 + 0.18 * jax.random.normal(streams_of[3], (CHANNELS,), jnp.float32), 0.1, 1.9),
        "norm_bias": gaussian(streams_of[4], (CHANNELS,), 0.5, 3.0, ((0, 2),), jnp.float32),
        "proj_weight": gaussian(streams_of[5], (CHANNELS, MODEL), CHANNELS ** -0.5, 0.125, ((0, 2), (1, 16))),
        "out_grad": heavy_noise(streams_of[6], (TOKENS, MODEL), 1.0, 6.0, ((0, 16),), (0, 1, 16, 2.0)),
    }


def reference(value_in, gate_in, taps, norm_gain, norm_bias, proj_weight, out_grad):
    f32 = jnp.float32
    rows = value_in.shape[0]
    span = taps.shape[0]
    half = span // 2
    width_all = value_in.shape[1]
    gate_sig = jax.nn.sigmoid(gate_in.astype(f32))
    value_f = value_in.astype(f32)
    mixed = (value_f * gate_sig).astype(jnp.bfloat16)
    padded = jnp.pad(mixed.astype(f32), ((half, half), (0, 0)))
    conv = jnp.zeros((rows, width_all), f32)
    for k in range(span):
        conv = conv + taps[k] * padded[k:k + rows]
    mean = lax.optimization_barrier(jnp.sum(conv, axis=1)) / width_all
    centred = conv - mean[:, None]
    spread = lax.optimization_barrier(jnp.sum(centred * centred, axis=1)) / width_all
    inv = lax.rsqrt(spread + 1e-06)
    normed = centred * inv[:, None]
    pre = normed * norm_gain + norm_bias
    act = jax.nn.silu(pre).astype(jnp.bfloat16)
    act_grad = lax.dot_general(out_grad, proj_weight, (((1,), (1,)), ((), ())), preferred_element_type=f32)
    weight_grad = lax.dot_general(act, out_grad, (((0,), (0,)), ((), ())), preferred_element_type=f32)
    sig_pre = jax.nn.sigmoid(pre)
    pre_grad = act_grad * sig_pre * (1.0 + pre * (1.0 - sig_pre))
    gain_grad = lax.optimization_barrier(jnp.sum(pre_grad * normed, axis=0))
    bias_grad = lax.optimization_barrier(jnp.sum(pre_grad, axis=0))
    normed_grad = pre_grad * norm_gain
    first = lax.optimization_barrier(jnp.sum(normed_grad, axis=1)) / width_all
    second = lax.optimization_barrier(jnp.sum(normed_grad * normed, axis=1)) / width_all
    conv_grad = inv[:, None] * (normed_grad - first[:, None] - normed * second[:, None])
    tap_grad = jnp.stack([lax.optimization_barrier(jnp.sum(conv_grad * padded[k:k + rows], axis=0)) for k in range(span)])
    grad_pad = jnp.pad(conv_grad, ((half, half), (0, 0)))
    mixed_grad = jnp.zeros((rows, width_all), f32)
    for k in range(span):
        mixed_grad = mixed_grad + taps[k] * grad_pad[2 * half - k:2 * half - k + rows]
    value_grad = (mixed_grad * gate_sig).astype(jnp.bfloat16)
    gate_grad = (mixed_grad * value_f * gate_sig * (1.0 - gate_sig)).astype(jnp.bfloat16)
    return (value_grad, gate_grad, tap_grad, gain_grad, bias_grad, weight_grad)
```

```python
import functools
import jax
import jax.numpy as jnp
from jax import lax
from jax.experimental import pallas as pl
from jax.experimental.pallas import tpu as pltpu
from jax.sharding import PartitionSpec as P


def padded_rows(cells, width):
    count = lax.axis_size("sp")
    ends = count - 1
    rows = cells.shape[0]
    before = lax.ppermute(cells[rows - width :], "sp", [(i, i + 1) for i in range(ends)])
    after = lax.ppermute(cells[:width], "sp", [(i + 1, i) for i in range(ends)])
    return jnp.concatenate([before, cells, after], axis=0)


def on_device(*arrays):
    return compute(*arrays)


def compute(value_in, gate_in, taps, norm_gain, norm_bias, proj_weight, out_grad):
    f32, bf16 = jnp.float32, jnp.bfloat16
    rows, local_width = value_in.shape
    span = taps.shape[0]
    half = span // 2
    tp = lax.axis_size("tp")
    count = lax.axis_size("sp")
    inner = 1 << ((count.bit_length() - 1) // 2)
    outer = count // inner
    width_all = local_width * tp
    block = proj_weight.shape[1]
    me = lax.axis_index("sp")
    plane, place = me // inner, me % inner
    core = lax.axis_index("tp")

    def swap(array, d):
        return lax.ppermute(
            array, "sp", [(i, i - i % inner + ((i % inner) ^ d)) for i in range(count)]
        )

    def shift(array, e):
        return lax.ppermute(array, "sp", [(i, (i + e * inner) % count) for i in range(count)])

    def across(array, t):
        return lax.ppermute(array, "tp", [(c, c ^ t) for c in range(tp)])

    def tp_sum(array):
        return array + sum(across(array, t) for t in range(1, tp))

    gate_sig = jax.nn.sigmoid(gate_in.astype(f32))
    value_f = value_in.astype(f32)
    mixed = (value_f * gate_sig).astype(bf16)
    padded = padded_rows(mixed, half).astype(f32)

    def columns_of(where, first, blocks):
        return jnp.concatenate(
            [
                lax.dynamic_slice_in_dim(
                    out_grad,
                    (((plane + first + e) % outer) * inner + where) * block,
                    block,
                    axis=1,
                )
                for e in range(blocks)
            ],
            axis=1,
        )

    share = outer // tp
    own_columns = columns_of(place, 0, outer)
    arrived = [swap(columns_of(place ^ d, core * share, share), d) for d in range(1, inner)]
    weights = [proj_weight] + [shift(proj_weight, -e) for e in range(1, outer)]
    weight_cols = jnp.concatenate(weights, axis=1)
    cotangents = [own_columns]
    for got in arrived:
        parts = jnp.stack([got] + [across(got, t) for t in range(1, tp)])
        cotangents.append(
            jnp.concatenate(
                [
                    lax.dynamic_index_in_dim(parts, core ^ j, axis=0, keepdims=False)
                    for j in range(tp)
                ],
                axis=1,
            )
        )

    conv = jnp.zeros((rows, local_width), f32)
    for k in range(span):
        conv = conv + taps[k] * padded[k : k + rows]
    mean = tp_sum(jnp.sum(conv, axis=1)) / width_all
    centred = conv - mean[:, None]
    spread = tp_sum(jnp.sum(centred * centred, axis=1)) / width_all
    inv = lax.rsqrt(spread + 1e-06)
    normed = centred * inv[:, None]
    pre = normed * norm_gain + norm_bias
    sig_pre = jax.nn.sigmoid(pre)
    act = (pre * sig_pre).astype(bf16)
    acts = [act] + [swap(act, d) for d in range(1, inner)]

    partial = [
        lax.dot_general(c, weight_cols, (((1,), (1,)), ((), ())), preferred_element_type=f32)
        for c in cotangents
    ]
    act_grad = partial[0]
    sending = lax.optimization_barrier(([p.astype(bf16) for p in partial[1:]], acts))[0]
    for d in range(1, inner):
        got = swap(sending[d - 1], d)
        act_grad = act_grad + got.astype(f32)

    pre_grad = act_grad * sig_pre * (1.0 + pre * (1.0 - sig_pre))
    normed_grad = pre_grad * norm_gain
    sums = tp_sum(
        jnp.stack([jnp.sum(normed_grad, axis=1), jnp.sum(normed_grad * normed, axis=1)])
    )
    first, second = sums[0], sums[1]
    conv_grad = inv[:, None] * (
        normed_grad - first[:, None] / width_all - normed * second[:, None] / width_all
    )
    extended = lax.optimization_barrier(padded_rows(conv_grad, half))
    tap_local = jnp.stack([jnp.sum(conv_grad * padded[k : k + rows], axis=0) for k in range(span)])
    gain_local = jnp.sum(pre_grad * normed, axis=0)
    bias_local = jnp.sum(pre_grad, axis=0)
    small = jnp.concatenate([tap_local, gain_local[None], bias_local[None]], axis=0)
    small = small + sum(swap(small, d) for d in range(1, inner))
    small = small + sum(shift(small, e) for e in range(1, outer))
    tap_grad, gain_grad, bias_grad = small[:span], small[span], small[span + 1]

    mixed_grad = jnp.zeros((rows, local_width), f32)
    for k in range(span):
        mixed_grad = mixed_grad + taps[k] * extended[2 * half - k : 2 * half - k + rows]
    value_grad = (mixed_grad * gate_sig).astype(bf16)
    gate_grad = (mixed_grad * value_f * gate_sig * (1.0 - gate_sig)).astype(bf16)

    weight_part = lax.dot_general(
        jnp.concatenate(acts, axis=0),
        jnp.concatenate(cotangents, axis=0),
        (((0,), (0,)), ((), ())),
        preferred_element_type=f32,
    )
    weight_grad = weight_part[:, :block]
    for e in range(1, outer):
        sent = weight_part[:, e * block : (e + 1) * block].astype(bf16)
        got = shift(sent, e)
        weight_grad = weight_grad + got.astype(f32)
    return (value_grad, gate_grad, tap_grad, gain_grad, bias_grad, weight_grad)


LANES = 128
EDGE = 16
MESH = pl.DeviceIdType.MESH


def slot_table(planes, blocks):
    parts = blocks // 2
    sizes = {
        "halo": 2,
        "cols_x": parts,
        "cols_x_core": parts,
        "cols_d": parts,
        "cols_d_core": parts,
        "cols_y": parts,
        "cols_y_core": parts,
        "w_y": 1,
        "w_up": 2 * (planes - 1),
        "w_down": 2 * (planes - 1),
        "stats": 1,
        "act_x": 1,
        "act_y": 1,
        "act_d": 1,
        "part_x": 2,
        "part_y": 1,
        "up": blocks,
        "down": blocks,
        "w_back": 1,
        "norm": 1,
        "grad_halo": 2,
        "plane_in": 3,
        "across": planes,
        "plane_out": 3,
    }
    first, total = {}, 0
    for name, size in sizes.items():
        first[name] = total
        total += size
    return first, total


def kernel(
    shape,
    first,
    value,
    gate,
    taps,
    gain,
    bias,
    weight,
    cotangent,
    value_grad,
    gate_grad,
    tap_grad,
    gain_grad,
    bias_grad,
    weight_grad,
    value_v,
    gate_v,
    cols,
    wh,
    tap_t,
    mixed,
    edge_out,
    edge_in,
    conv,
    dact,
    stat_out,
    stat_in,
    rows_of,
    acts,
    factor_v,
    factor_g,
    part,
    part_out,
    part_in,
    half_out,
    half_in,
    wg,
    up_out,
    down_out,
    up_in,
    down_in,
    back_out,
    back_in,
    grads,
    gedge_out,
    gedge_in,
    small,
    plane_in,
    across,
    owned,
    small_all,
    tile,
    send_sem,
    recv_sem,
    local_sem,
):
    rows, width, span, planes, block, step = shape
    f32, bf16 = jnp.float32, jnp.bfloat16
    blocks = 2 * planes
    parts = blocks // 2
    side = width // 2
    tiles = width // LANES
    tiles_side = tiles // 2
    quarter = tiles // 4
    count = 4 * planes
    half = span // 2
    lead = EDGE - half

    me, core = lax.axis_index("sp"), lax.axis_index("tp")
    z, y, x = lax.div(me, 4), lax.rem(lax.div(me, 2), 2), lax.rem(me, 2)
    yn, xn = 1 - y, 1 - x

    def at(zz, yy, xx):
        return (zz * 4 + yy * 2 + xx, core)

    to_x, to_y, to_d = at(z, y, xn), at(z, yn, x), at(z, yn, xn)
    to_core = (me, 1 - core)
    to_up, to_down = (me + 4, core), (me - 4, core)
    to_next, to_prev = (me + 1, core), (me - 1, core)
    has_up, has_down = z < planes - 1, z > 0
    has_next, has_prev = me < count - 1, me > 0

    pending = []

    def copy(src, dst, name, index, device):
        at_slot = first[name] + index
        return pltpu.make_async_remote_copy(
            src_ref=src,
            dst_ref=dst,
            send_sem=send_sem.at[at_slot],
            recv_sem=recv_sem.at[at_slot],
            device_id=device,
            device_id_type=MESH,
        )

    def send(made, when=None):
        pending.append((made, when))
        if when is None:
            made.start()
        else:
            pl.when(when)(made.start)

    def arrive(made, when=None):
        if when is None:
            made.wait_recv()
        else:
            pl.when(when)(made.wait_recv)

    def lanes(j):
        return pl.ds(pl.multiple_of(j * LANES, LANES), LANES)

    def over(n, body):
        def step_of(j, carry):
            body(j)
            return carry

        lax.fori_loop(0, n, step_of, 0)

    my_rows = pl.ds(pl.multiple_of(y * side, side), side)
    their_rows = pl.ds(pl.multiple_of(yn * side, side), side)

    def column(b):
        return pl.ds(pl.multiple_of(b * block, block), block)

    def index_of(c, q):
        return c * (blocks - 1) + q * (1 - 2 * c)

    mine = [index_of(core, q) for q in range(parts)]
    other = [index_of(1 - core, q) for q in range(parts)]

    load_v = pltpu.make_async_copy(value, value_v, local_sem.at[0])
    load_g = pltpu.make_async_copy(gate, gate_v, local_sem.at[1])
    load_w = pltpu.make_async_copy(weight.at[my_rows], wh.at[z * 2 + y], local_sem.at[2])
    load_c = [
        pltpu.make_async_copy(
            cotangent.at[:, column(2 * i + x)], cols.at[0, i], local_sem.at[3 + i]
        )
        for i in range(blocks)
    ]
    load_v.start()
    load_g.start()

    barrier = pltpu.get_barrier_semaphore()
    peers = [to_x, to_y, to_d, to_core]
    peers += [at(lax.rem(z + d, planes), y, x) for d in range(1, planes)]
    peers += [(lax.rem(me + 1, count), core), (lax.rem(me + count - 1, count), core)]
    for peer in peers:
        pl.semaphore_signal(barrier, inc=1, device_id=peer, device_id_type=MESH)
    pl.semaphore_wait(barrier, len(peers))

    def w_copies(d, p):
        yb = y if p == 0 else yn
        index = 2 * (d - 1) + p
        below = wh.at[lax.rem(z - d + planes, planes) * 2 + yb]
        above = wh.at[lax.rem(z + d, planes) * 2 + yb]
        return (
            copy(below, below, "w_up", index, to_up),
            copy(above, above, "w_down", index, to_down),
        )

    def w_first(p, src, yb):
        dst = wh.at[z * 2 + yb]
        send(copy(src, dst, "w_up", p, to_up), has_up)
        send(copy(src, dst, "w_down", p, to_down), has_down)

    def w_forward(d, p):
        up, down = w_copies(d, p)
        yb = y if p == 0 else yn
        below = wh.at[lax.rem(z - d + planes, planes) * 2 + yb]
        above = wh.at[lax.rem(z + d, planes) * 2 + yb]
        arrive(up, z >= d)
        if d < planes - 1:
            send(copy(below, below, "w_up", 2 * d + p, to_up), jnp.logical_and(z >= d, has_up))
        arrive(down, z + d < planes)
        if d < planes - 1:
            send(
                copy(above, above, "w_down", 2 * d + p, to_down),
                jnp.logical_and(z + d < planes, has_down),
            )

    w_first(0, weight.at[my_rows], y)
    w_y = copy(weight.at[their_rows], wh.at[z * 2 + y], "w_y", 0, to_y)
    send(w_y)

    def cols_x(q):
        return copy(
            cotangent.at[:, column(2 * mine[q] + xn)], cols.at[1, mine[q]], "cols_x", q, to_x
        )

    def cols_d(q):
        return copy(cols.at[1, mine[q]], cols.at[3, mine[q]], "cols_d", q, to_y)

    def cols_y(q):
        return copy(
            cotangent.at[:, column(2 * mine[q] + x)], cols.at[2, mine[q]], "cols_y", q, to_y
        )

    def cols_core(slab, name, q):
        ref = cols.at[slab, mine[q]]
        return copy(ref, ref, name, q, to_core)

    def pass_x(q):
        arrive(cols_x(q))
        send(cols_d(q))
        send(cols_core(1, "cols_x_core", q))

    def pass_d(q):
        arrive(cols_d(q))
        send(cols_core(3, "cols_d_core", q))

    def pass_y(q):
        arrive(cols_y(q))
        send(cols_core(2, "cols_y_core", q))

    send(cols_x(0))

    def lay_taps(j):
        tap_t[j, 0:span, :] = taps[:, lanes(j)]
        small[j] = jnp.zeros(small.shape[1:], f32)

    over(tiles, lay_taps)
    load_v.wait()
    load_g.wait()

    def gate_tile(j):
        sig = jax.nn.sigmoid(gate_v[:, lanes(j)].astype(f32))
        got = (value_v[:, lanes(j)].astype(f32) * sig).astype(bf16).astype(f32)
        mixed[j, EDGE : EDGE + rows, :] = got
        edge_out[0, j] = mixed[j, rows : rows + EDGE, :].astype(bf16)
        edge_out[1, j] = mixed[j, EDGE : 2 * EDGE, :].astype(bf16)

    over(tiles, gate_tile)
    halo_prev = copy(edge_out.at[0], edge_in.at[0], "halo", 0, to_next)
    halo_next = copy(edge_out.at[1], edge_in.at[1], "halo", 1, to_prev)
    send(halo_prev, has_next)
    send(halo_next, has_prev)
    for q in range(1, parts):
        send(cols_x(q))
    load_w.start()
    for made in load_c:
        made.start()

    def fill(made, when, src, dst, at_row):
        @pl.when(when)
        def _():
            made.wait_recv()
            for j in range(tiles):
                dst[j, at_row : at_row + EDGE, :] = src[j].astype(f32)

        @pl.when(jnp.logical_not(when))
        def _():
            for j in range(tiles):
                dst[j, at_row : at_row + EDGE, :] = jnp.zeros((EDGE, LANES), f32)

    fill(halo_prev, has_prev, edge_in.at[0], mixed, 0)
    fill(halo_next, has_next, edge_in.at[1], mixed, EDGE + rows)

    def conv_tile(j):
        for r in range(0, rows, step):
            acc = tap_t[j, 0:1, :] * mixed[j, r + lead : r + lead + step, :]
            for k in range(1, span):
                at_row = r + k + lead
                acc = acc + tap_t[j, k : k + 1, :] * mixed[j, at_row : at_row + step, :]
            conv[j, r : r + step, :] = acc

    over(tiles, conv_tile)
    pass_x(0)
    arrive(w_y)
    w_first(1, wh.at[z * 2 + yn], yn)
    w_forward(1, 0)

    for r in range(0, rows, step):
        at_rows = slice(r, r + step)
        total = conv[0, at_rows, :]
        for j in range(1, tiles):
            total = total + conv[j, at_rows, :]
        middle = jnp.sum(total, axis=1, keepdims=True) / width
        off = conv[0, at_rows, :] - middle
        square = off * off
        for j in range(1, tiles):
            off = conv[j, at_rows, :] - middle
            square = square + off * off
        stat_out[0, at_rows, :] = total
        stat_out[1, at_rows, :] = square
    stats = copy(stat_out.at[0:2], stat_in.at[0:2], "stats", 0, to_core)
    send(stats)
    pass_x(1) if parts > 1 else None
    arrive(stats)
    for r in range(0, rows, step):
        at_rows = slice(r, r + step)
        here = jnp.sum(stat_out[0, at_rows, :], axis=1, keepdims=True)
        there = jnp.sum(stat_in[0, at_rows, :], axis=1, keepdims=True)
        both = stat_out[1, at_rows, :] + stat_in[1, at_rows, :]
        apart = (here - there) / width
        spread = jnp.sum(both, axis=1, keepdims=True) / (2 * width) + apart * apart / 4
        inv = lax.rsqrt(spread + 1e-06)
        rows_of[0, at_rows, :] = jnp.broadcast_to((here + there) / (2 * width), (step, LANES))
        rows_of[1, at_rows, :] = jnp.broadcast_to(inv, (step, LANES))

    def act_side(h):
        def act_tile(jj):
            j = h * tiles_side + jj
            normed = (conv[j] - rows_of[0]) * rows_of[1]
            pre = normed * gain[0:1, lanes(j)] + bias[0:1, lanes(j)]
            sig = jax.nn.sigmoid(pre)
            acts[h, :, lanes(jj)] = (pre * sig).astype(bf16)
            conv[j] = normed
            dact[j] = sig * (1.0 + pre * (1.0 - sig))

        over(tiles_side, act_tile)

    act_y = copy(acts.at[yn], acts.at[3], "act_y", 0, to_y)
    act_x = copy(acts.at[y], acts.at[2], "act_x", 0, to_x)
    act_d = copy(acts.at[3], acts.at[4], "act_d", 0, to_x)
    act_side(yn)
    send(act_y)
    act_side(y)
    send(act_x)
    w_forward(1, 1)
    for q in range(2, parts):
        pass_x(q)
    for q in range(parts):
        send(cols_y(q))
    if planes > 2:
        w_forward(2, 0)

    def factor_tile(j):
        sig = jax.nn.sigmoid(gate_v[:, lanes(j)].astype(f32))
        factor_v[j] = sig
        factor_g[j] = value_v[:, lanes(j)].astype(f32) * sig * (1.0 - sig)

    over(tiles, factor_tile)
    if planes > 2:
        w_forward(2, 1)
    arrive(act_y)
    send(act_d)
    for d in range(3, planes):
        w_forward(d, 0)
    for q in range(parts):
        pass_d(q)
    for d in range(3, planes):
        w_forward(d, 1)
    load_w.wait()
    for made in load_c:
        made.wait()

    def product(slab):
        def one(i):
            got = lax.dot_general(
                cols[slab, i], wh[i], (((1,), (1,)), ((), ())), preferred_element_type=f32
            )
            part[slab] = part[slab] + got

        part[slab] = lax.dot_general(
            cols[slab, 0], wh[0], (((1,), (1,)), ((), ())), preferred_element_type=f32
        )
        lax.fori_loop(1, blocks, lambda i, c: (one(i), c)[1], 0)

    part_x = [copy(part_out.at[n], part_in.at[n], "part_x", n, to_x) for n in range(2)]

    def partial(slab, n):
        product(slab)
        part_out[n] = part[slab].astype(bf16)
        send(part_x[n])

    for q in range(parts):
        arrive(cols_core(3, "cols_d_core", q))
    partial(3, 1)
    for q in range(parts):
        arrive(cols_core(1, "cols_x_core", q))
    partial(1, 0)

    arrive(act_x)
    arrive(act_d)

    def weight_of(i):
        acc = None
        for slab, where in enumerate((y, 2, 3, 4)):
            got = lax.dot_general(
                acts[where],
                cols[slab, i],
                (((0,), (0,)), ((), ())),
                preferred_element_type=f32,
            )
            acc = got if acc is None else acc + got
        wg[i] = acc

    for q in range(parts):
        pass_y(q)
        weight_of(mine[q])
        arrive(cols_core(2, "cols_y_core", q))
        weight_of(other[q])

    def up_copy(t, p):
        i = 2 * t + (yn if p == 0 else y)
        return copy(up_out.at[i], up_in.at[i], "up", 2 * t + p, to_up)

    def down_copy(t, p):
        i = 2 * t + (yn if p == 0 else y)
        return copy(down_out.at[i], down_in.at[i], "down", 2 * t + p, to_down)

    def relay(t, p, made, out, got, going, fresh):
        i = 2 * t + (yn if p == 0 else y)

        @pl.when(jnp.logical_and(going, fresh))
        def _():
            out[i] = wg[i].astype(bf16)

        @pl.when(jnp.logical_and(going, jnp.logical_not(fresh)))
        def _():
            made.wait_recv()
            out[i] = (wg[i] + got[i].astype(f32)).astype(bf16)

        send(made, going)

    def serve(m, p):
        t = planes - 1 - m
        relay(t, p, up_copy(t, p), up_out, up_in, z < t, z == 0)
        relay(m, p, down_copy(m, p), down_out, down_in, z > m, z == planes - 1)

    product(2)
    serve(0, 0)
    arrive(part_x[1])
    half_out[...] = (part[2] + part_in[1].astype(f32)).astype(bf16)
    part_y = copy(half_out, half_in, "part_y", 0, to_y)
    send(part_y)
    product(0)
    serve(0, 1)
    arrive(part_x[0])

    stat_out[2] = jnp.zeros((rows, LANES), f32)
    stat_out[3] = jnp.zeros((rows, LANES), f32)

    def back_tile(j, got):
        pre_grad = got * dact[j]
        normed = conv[j]
        scaled = pre_grad * gain[0:1, lanes(j)]
        crossed = pre_grad * normed
        dact[j] = scaled
        stat_out[2] = stat_out[2] + scaled
        stat_out[3] = stat_out[3] + scaled * normed
        small[j, span : span + 1, :] = jnp.sum(crossed, axis=0, keepdims=True)
        small[j, span + 1 : span + 2, :] = jnp.sum(pre_grad, axis=0, keepdims=True)

    def back_mine(jj):
        got = part[0, :, lanes(jj)] + part_in[0, :, lanes(jj)].astype(f32)
        back_tile(y * tiles_side + jj, got)

    def back_theirs(jj):
        back_tile(yn * tiles_side + jj, half_in[:, lanes(jj)].astype(f32))

    over(tiles_side, back_mine)
    arrive(part_y)
    over(tiles_side, back_theirs)
    norm = copy(stat_out.at[2:4], stat_in.at[2:4], "norm", 0, to_core)
    send(norm)
    if planes > 2:
        serve(1, 0)
    arrive(norm)
    for r in range(0, rows, step):
        at_rows = slice(r, r + step)
        for n in range(2):
            both = stat_out[2 + n, at_rows, :] + stat_in[2 + n, at_rows, :]
            got = jnp.sum(both, axis=1, keepdims=True) / (2 * width)
            rows_of[2 + n, at_rows, :] = jnp.broadcast_to(got, (step, LANES))

    def grad_tile(j):
        grads[j, EDGE : EDGE + rows, :] = rows_of[1] * (
            dact[j] - rows_of[2] - conv[j] * rows_of[3]
        )
        gedge_out[0, j] = grads[j, rows : rows + EDGE, :]
        gedge_out[1, j] = grads[j, EDGE : 2 * EDGE, :]

    over(tiles, grad_tile)
    grad_prev = copy(gedge_out.at[0], gedge_in.at[0], "grad_halo", 0, to_next)
    grad_next = copy(gedge_out.at[1], gedge_in.at[1], "grad_halo", 1, to_prev)
    send(grad_prev, has_next)
    send(grad_next, has_prev)

    def tap_tile(j):
        def block_of(r, acc):
            base = pl.multiple_of(r * step, 8)
            own = grads[j, pl.ds(base + EDGE, step), :]
            out = []
            for k in range(span):
                got = own * mixed[j, pl.ds(base + k + lead, step), :]
                out.append(acc[k] + jnp.sum(got.reshape(step // 8, 8, LANES), axis=0))
            return tuple(out)

        start = tuple(jnp.zeros((8, LANES), f32) for _ in range(span))
        acc = lax.fori_loop(0, rows // step, block_of, start)
        for k in range(span):
            small[j, k : k + 1, :] = jnp.sum(acc[k], axis=0, keepdims=True)

    over(tiles, tap_tile)

    place = 2 * y + x
    near = [(to_x, 2 * y + xn), (to_y, 2 * yn + x), (to_d, 2 * yn + xn)]
    own_tiles = pl.ds(place * quarter, quarter)
    gather = [
        copy(small.at[pl.ds(p * quarter, quarter)], plane_in.at[n], "plane_in", n, dev)
        for n, (dev, p) in enumerate(near)
    ]
    for made in gather:
        send(made)
    if planes > 2:
        serve(1, 1)
    fill(grad_prev, has_prev, gedge_in.at[0], grads, 0)
    fill(grad_next, has_next, gedge_in.at[1], grads, EDGE + rows)

    def mixed_tile(j):
        for r in range(0, rows, step):
            at_row = r + EDGE + half
            acc = tap_t[j, 0:1, :] * grads[j, at_row : at_row + step, :]
            for k in range(1, span):
                at_row = r + EDGE + half - k
                acc = acc + tap_t[j, k : k + 1, :] * grads[j, at_row : at_row + step, :]
            tile[r : r + step, :] = acc
        got = tile[...]
        value_grad[:, lanes(j)] = (got * factor_v[j]).astype(bf16)
        gate_grad[:, lanes(j)] = (got * factor_g[j]).astype(bf16)

    def mixed_tiles(lo, hi):
        lax.fori_loop(lo, hi, lambda j, c: (mixed_tile(j), c)[1], 0)

    mixed_tiles(0, tiles_side)
    for made in gather:
        arrive(made)
    across[z] = small[own_tiles] + plane_in[0] + plane_in[1] + plane_in[2]
    for d in range(1, planes):
        made = copy(across.at[z], across.at[z], "across", d, at(lax.rem(z + d, planes), y, x))
        send(made)
    for m in range(2, planes - 1):
        serve(m, 0)
    mixed_tiles(tiles_side, tiles)
    for d in range(1, planes):
        arrive(copy(across.at[z], across.at[z], "across", d, to_core))
    total = across[0]
    for d in range(1, planes):
        total = total + across[d]
    owned[...] = total
    small_all[own_tiles] = total
    spread_out = [
        copy(owned, small_all.at[own_tiles], "plane_out", n, dev) for n, (dev, p) in enumerate(near)
    ]
    for made in spread_out:
        send(made)
    for m in range(2, planes - 1):
        serve(m, 1)

    def finish(p):
        i = 2 * z + (yn if p == 0 else y)
        for t in range(planes):

            @pl.when(z == t)
            def _():
                total = wg[i]
                if t > 0:
                    up_copy(t, p).wait_recv()
                    total = total + up_in[i].astype(f32)
                if t < planes - 1:
                    down_copy(t, p).wait_recv()
                    total = total + down_in[i].astype(f32)
                if p == 0:
                    back_out[...] = total.astype(bf16)
                else:
                    weight_grad[my_rows, :] = total

    finish(0)
    back = copy(back_out, back_in, "w_back", 0, to_y)
    send(back)
    for made in spread_out:
        arrive(made)
    for j in range(tiles):
        tap_grad[:, j * LANES : (j + 1) * LANES] = small_all[j, 0:span, :]
        gain_grad[:, j * LANES : (j + 1) * LANES] = small_all[j, span : span + 1, :]
        bias_grad[:, j * LANES : (j + 1) * LANES] = small_all[j, span + 1 : span + 2, :]
    finish(1)
    arrive(back)
    weight_grad[their_rows, :] = back_in[...].astype(f32)
    for made, when in pending:
        if when is None:
            made.wait_send()
        else:
            pl.when(when)(made.wait_send)


def fused_on_device(value_in, gate_in, taps, norm_gain, norm_bias, proj_weight, out_grad):
    f32, bf16 = jnp.float32, jnp.bfloat16
    rows, width = value_in.shape
    span = taps.shape[0]
    block = proj_weight.shape[1]
    planes = lax.axis_size("sp") // 4
    blocks = 2 * planes
    side = width // 2
    tiles = width // LANES
    step = max(n for n in (8, 16, 24, 32, 40) if rows % n == 0)
    kept = -(-(span + 2) // 8) * 8
    first, total = slot_table(planes, blocks)
    vmem, dma = pltpu.VMEM, pltpu.SemaphoreType.DMA
    scratch = [
        vmem((rows, width), bf16),
        vmem((rows, width), bf16),
        vmem((4, blocks, rows, block), bf16),
        vmem((blocks, side, block), bf16),
        vmem((tiles, kept, LANES), f32),
        vmem((tiles, rows + 2 * EDGE, LANES), f32),
        vmem((2, tiles, EDGE, LANES), bf16),
        vmem((2, tiles, EDGE, LANES), bf16),
        vmem((tiles, rows, LANES), f32),
        vmem((tiles, rows, LANES), f32),
        vmem((4, rows, LANES), f32),
        vmem((4, rows, LANES), f32),
        vmem((4, rows, LANES), f32),
        vmem((5, rows, side), bf16),
        vmem((tiles, rows, LANES), f32),
        vmem((tiles, rows, LANES), f32),
        vmem((4, rows, side), f32),
        vmem((2, rows, side), bf16),
        vmem((2, rows, side), bf16),
        vmem((rows, side), bf16),
        vmem((rows, side), bf16),
        vmem((blocks, side, block), f32),
        vmem((blocks, side, block), bf16),
        vmem((blocks, side, block), bf16),
        vmem((blocks, side, block), bf16),
        vmem((blocks, side, block), bf16),
        vmem((side, block), bf16),
        vmem((side, block), bf16),
        vmem((tiles, rows + 2 * EDGE, LANES), f32),
        vmem((2, tiles, EDGE, LANES), f32),
        vmem((2, tiles, EDGE, LANES), f32),
        vmem((tiles, kept, LANES), f32),
        vmem((3, tiles // 4, kept, LANES), f32),
        vmem((planes, tiles // 4, kept, LANES), f32),
        vmem((tiles // 4, kept, LANES), f32),
        vmem((tiles, kept, LANES), f32),
        vmem((rows, LANES), f32),
        dma((total,)),
        dma((total,)),
        dma((3 + blocks,)),
    ]
    whole, hbm = pl.BlockSpec(memory_space=pltpu.VMEM), pl.BlockSpec(memory_space=pl.ANY)
    outs = pl.pallas_call(
        functools.partial(kernel, (rows, width, span, planes, block, step), first),
        out_shape=(
            jax.ShapeDtypeStruct((rows, width), bf16),
            jax.ShapeDtypeStruct((rows, width), bf16),
            jax.ShapeDtypeStruct((span, width), f32),
            jax.ShapeDtypeStruct((1, width), f32),
            jax.ShapeDtypeStruct((1, width), f32),
            jax.ShapeDtypeStruct((width, block), f32),
        ),
        in_specs=[hbm, hbm, whole, whole, whole, hbm, hbm],
        out_specs=[whole] * 6,
        scratch_shapes=scratch,
        compiler_params=pltpu.CompilerParams(
            collective_id=0, has_side_effects=True, vmem_limit_bytes=62 * 2**20
        ),
    )(
        value_in,
        gate_in,
        taps,
        norm_gain.reshape(1, width),
        norm_bias.reshape(1, width),
        proj_weight,
        out_grad,
    )
    value_grad, gate_grad, tap_grad, gain_grad, bias_grad, weight_grad = outs
    return (
        value_grad,
        gate_grad,
        tap_grad,
        gain_grad.reshape(width),
        bias_grad.reshape(width),
        weight_grad,
    )


def solution(mesh):
    fused = mesh.shape["tp"] == 2 and mesh.shape["sp"] % 4 == 0
    return jax.shard_map(
        fused_on_device if fused else on_device,
        mesh=mesh,
        in_specs=(
            P("sp", "tp"),
            P("sp", "tp"),
            P(None, "tp"),
            P("tp"),
            P("tp"),
            P("tp", "sp"),
            P("sp", None),
        ),
        out_specs=(P("sp", "tp"), P("sp", "tp"), P(None, "tp"), P("tp"), P("tp"), P("tp", "sp")),
        check_vma=False,
    )
```

```python
import functools
import jax
import jax.numpy as jnp
from jax import lax
from jax.experimental import pallas as pl
from jax.experimental.pallas import tpu as pltpu
from jax.sharding import PartitionSpec as P


def padded_rows(cells, width):
    count = lax.axis_size("sp")
    ends = count - 1
    rows = cells.shape[0]
    before = lax.ppermute(cells[rows - width :], "sp", [(i, i + 1) for i in range(ends)])
    after = lax.ppermute(cells[:width], "sp", [(i + 1, i) for i in range(ends)])
    return jnp.concatenate([before, cells, after], axis=0)


def on_device(*arrays):
    return compute(*arrays)


def compute(value_in, gate_in, taps, norm_gain, norm_bias, proj_weight, out_grad):
    f32, bf16 = jnp.float32, jnp.bfloat16
    rows, local_width = value_in.shape
    span = taps.shape[0]
    half = span // 2
    tp = lax.axis_size("tp")
    count = lax.axis_size("sp")
    inner = 1 << ((count.bit_length() - 1) // 2)
    outer = count // inner
    width_all = local_width * tp
    block = proj_weight.shape[1]
    me = lax.axis_index("sp")
    plane, place = me // inner, me % inner
    core = lax.axis_index("tp")

    def swap(array, d):
        return lax.ppermute(
            array, "sp", [(i, i - i % inner + ((i % inner) ^ d)) for i in range(count)]
        )

    def shift(array, e):
        return lax.ppermute(array, "sp", [(i, (i + e * inner) % count) for i in range(count)])

    def across(array, t):
        return lax.ppermute(array, "tp", [(c, c ^ t) for c in range(tp)])

    def tp_sum(array):
        return array + sum(across(array, t) for t in range(1, tp))

    gate_sig = jax.nn.sigmoid(gate_in.astype(f32))
    value_f = value_in.astype(f32)
    mixed = (value_f * gate_sig).astype(bf16)
    padded = padded_rows(mixed, half).astype(f32)

    def columns_of(where, first, blocks):
        return jnp.concatenate(
            [
                lax.dynamic_slice_in_dim(
                    out_grad,
                    (((plane + first + e) % outer) * inner + where) * block,
                    block,
                    axis=1,
                )
                for e in range(blocks)
            ],
            axis=1,
        )

    share = outer // tp
    own_columns = columns_of(place, 0, outer)
    arrived = [swap(columns_of(place ^ d, core * share, share), d) for d in range(1, inner)]
    weights = [proj_weight] + [shift(proj_weight, -e) for e in range(1, outer)]
    weight_cols = jnp.concatenate(weights, axis=1)
    cotangents = [own_columns]
    for got in arrived:
        parts = jnp.stack([got] + [across(got, t) for t in range(1, tp)])
        cotangents.append(
            jnp.concatenate(
                [
                    lax.dynamic_index_in_dim(parts, core ^ j, axis=0, keepdims=False)
                    for j in range(tp)
                ],
                axis=1,
            )
        )

    conv = jnp.zeros((rows, local_width), f32)
    for k in range(span):
        conv = conv + taps[k] * padded[k : k + rows]
    mean = tp_sum(jnp.sum(conv, axis=1)) / width_all
    centred = conv - mean[:, None]
    spread = tp_sum(jnp.sum(centred * centred, axis=1)) / width_all
    inv = lax.rsqrt(spread + 1e-06)
    normed = centred * inv[:, None]
    pre = normed * norm_gain + norm_bias
    sig_pre = jax.nn.sigmoid(pre)
    act = (pre * sig_pre).astype(bf16)
    acts = [act] + [swap(act, d) for d in range(1, inner)]

    partial = [
        lax.dot_general(c, weight_cols, (((1,), (1,)), ((), ())), preferred_element_type=f32)
        for c in cotangents
    ]
    act_grad = partial[0]
    sending = lax.optimization_barrier(([p.astype(bf16) for p in partial[1:]], acts))[0]
    for d in range(1, inner):
        got = swap(sending[d - 1], d)
        act_grad = act_grad + got.astype(f32)

    pre_grad = act_grad * sig_pre * (1.0 + pre * (1.0 - sig_pre))
    normed_grad = pre_grad * norm_gain
    sums = tp_sum(
        jnp.stack([jnp.sum(normed_grad, axis=1), jnp.sum(normed_grad * normed, axis=1)])
    )
    first, second = sums[0], sums[1]
    conv_grad = inv[:, None] * (
        normed_grad - first[:, None] / width_all - normed * second[:, None] / width_all
    )
    extended = lax.optimization_barrier(padded_rows(conv_grad, half))
    tap_local = jnp.stack([jnp.sum(conv_grad * padded[k : k + rows], axis=0) for k in range(span)])
    gain_local = jnp.sum(pre_grad * normed, axis=0)
    bias_local = jnp.sum(pre_grad, axis=0)
    small = jnp.concatenate([tap_local, gain_local[None], bias_local[None]], axis=0)
    small = small + sum(swap(small, d) for d in range(1, inner))
    small = small + sum(shift(small, e) for e in range(1, outer))
    tap_grad, gain_grad, bias_grad = small[:span], small[span], small[span + 1]

    mixed_grad = jnp.zeros((rows, local_width), f32)
    for k in range(span):
        mixed_grad = mixed_grad + taps[k] * extended[2 * half - k : 2 * half - k + rows]
    value_grad = (mixed_grad * gate_sig).astype(bf16)
    gate_grad = (mixed_grad * value_f * gate_sig * (1.0 - gate_sig)).astype(bf16)

    weight_part = lax.dot_general(
        jnp.concatenate(acts, axis=0),
        jnp.concatenate(cotangents, axis=0),
        (((0,), (0,)), ((), ())),
        preferred_element_type=f32,
    )
    weight_grad = weight_part[:, :block]
    for e in range(1, outer):
        sent = weight_part[:, e * block : (e + 1) * block].astype(bf16)
        got = shift(sent, e)
        weight_grad = weight_grad + got.astype(f32)
    return (value_grad, gate_grad, tap_grad, gain_grad, bias_grad, weight_grad)


LANES = 128
EDGE = 16
MESH = pl.DeviceIdType.MESH


def slot_table(planes, blocks):
    parts = blocks // 2
    sizes = {
        "halo": 2,
        "cols_x": parts,
        "cols_x_core": parts,
        "cols_d": parts,
        "cols_d_core": parts,
        "cols_y": parts,
        "cols_y_core": parts,
        "w_y": 1,
        "w_up": 2 * (planes - 1),
        "w_down": 2 * (planes - 1),
        "stats": 1,
        "act_x": 1,
        "act_y": 1,
        "act_d": 1,
        "part_x": 4,
        "part_y": 2,
        "up": blocks,
        "down": blocks,
        "w_back": 1,
        "norm": 1,
        "grad_halo": 2,
        "plane_in": 3,
        "across": planes,
        "plane_out": 3,
    }
    first, total = {}, 0
    for name, size in sizes.items():
        first[name] = total
        total += size
    return first, total


def kernel(
    shape,
    first,
    value,
    gate,
    taps,
    gain,
    bias,
    weight,
    cotangent,
    value_grad,
    gate_grad,
    tap_grad,
    gain_grad,
    bias_grad,
    weight_grad,
    value_v,
    gate_v,
    cols,
    wh,
    tap_t,
    mixed,
    edge_out,
    edge_in,
    conv,
    dact,
    stat_out,
    stat_in,
    rows_of,
    acts,
    factor_v,
    factor_g,
    part,
    part_out,
    part_in,
    half_out,
    half_in,
    wg,
    up_out,
    down_out,
    up_in,
    down_in,
    back_out,
    back_in,
    weight_v,
    turned,
    grads,
    gedge_out,
    gedge_in,
    small,
    plane_in,
    across,
    owned,
    small_all,
    tile,
    send_sem,
    recv_sem,
    local_sem,
):
    rows, width, span, planes, block, step = shape
    f32, bf16 = jnp.float32, jnp.bfloat16
    blocks = 2 * planes
    parts = blocks // 2
    side = width // 2
    tiles = width // LANES
    tiles_side = tiles // 2
    quarter = tiles // 4
    count = 4 * planes
    half = span // 2
    lead = EDGE - half

    me, core = lax.axis_index("sp"), lax.axis_index("tp")
    z, y, x = lax.div(me, 4), lax.rem(lax.div(me, 2), 2), lax.rem(me, 2)
    yn, xn = 1 - y, 1 - x

    def at(zz, yy, xx):
        return (zz * 4 + yy * 2 + xx, core)

    to_x, to_y, to_d = at(z, y, xn), at(z, yn, x), at(z, yn, xn)
    to_core = (me, 1 - core)
    to_up, to_down = (me + 4, core), (me - 4, core)
    to_next, to_prev = (me + 1, core), (me - 1, core)
    has_up, has_down = z < planes - 1, z > 0
    has_next, has_prev = me < count - 1, me > 0

    pending = []

    def copy(src, dst, name, index, device):
        at_slot = first[name] + index
        return pltpu.make_async_remote_copy(
            src_ref=src,
            dst_ref=dst,
            send_sem=send_sem.at[at_slot],
            recv_sem=recv_sem.at[at_slot],
            device_id=device,
            device_id_type=MESH,
        )

    def send(made, when=None):
        pending.append((made, when))
        if when is None:
            made.start()
        else:
            pl.when(when)(made.start)

    def arrive(made, when=None):
        if when is None:
            made.wait_recv()
        else:
            pl.when(when)(made.wait_recv)

    def lanes(j):
        return pl.ds(pl.multiple_of(j * LANES, LANES), LANES)

    def over(n, body):
        def step_of(j, carry):
            body(j)
            return carry

        lax.fori_loop(0, n, step_of, 0)

    my_rows = pl.ds(pl.multiple_of(y * side, side), side)
    their_rows = pl.ds(pl.multiple_of(yn * side, side), side)

    def column(b):
        return pl.ds(pl.multiple_of(b * block, block), block)

    def index_of(c, q):
        return c * (blocks - 1) + q * (1 - 2 * c)

    mine = [index_of(core, q) for q in range(parts)]

    def cols_at(slab, i):
        return cols.at[slab, lax.div(i, 2), :, column(lax.rem(i, 2))]

    def wh_at(zz, yy):
        return wh.at[zz, :, column(yy)]

    load_v = pltpu.make_async_copy(value, value_v, local_sem.at[0])
    load_g = pltpu.make_async_copy(gate, gate_v, local_sem.at[1])
    load_w = pltpu.make_async_copy(weight.at[my_rows], wh_at(z, y), local_sem.at[2])
    load_c = [
        pltpu.make_async_copy(
            cotangent.at[:, column(2 * i + x)],
            cols.at[0, i // 2, :, (i % 2) * block : (i % 2 + 1) * block],
            local_sem.at[3 + i],
        )
        for i in range(blocks)
    ]
    load_v.start()
    load_g.start()

    barrier = pltpu.get_barrier_semaphore()
    peers = [to_x, to_y, to_d, to_core]
    peers += [at(lax.rem(z + d, planes), y, x) for d in range(1, planes)]
    peers += [(lax.rem(me + 1, count), core), (lax.rem(me + count - 1, count), core)]
    for peer in peers:
        pl.semaphore_signal(barrier, inc=1, device_id=peer, device_id_type=MESH)

    def w_copies(d, p):
        yb = y if p == 0 else yn
        index = 2 * (d - 1) + p
        below = wh_at(lax.rem(z - d + planes, planes), yb)
        above = wh_at(lax.rem(z + d, planes), yb)
        return (
            copy(below, below, "w_up", index, to_up),
            copy(above, above, "w_down", index, to_down),
        )

    def w_first(p, src, yb):
        dst = wh_at(z, yb)
        send(copy(src, dst, "w_up", p, to_up), has_up)
        send(copy(src, dst, "w_down", p, to_down), has_down)

    def w_forward(d, p):
        up, down = w_copies(d, p)
        yb = y if p == 0 else yn
        below = wh_at(lax.rem(z - d + planes, planes), yb)
        above = wh_at(lax.rem(z + d, planes), yb)
        arrive(up, z >= d)
        if d < planes - 1:
            send(copy(below, below, "w_up", 2 * d + p, to_up), jnp.logical_and(z >= d, has_up))
        arrive(down, z + d < planes)
        if d < planes - 1:
            send(
                copy(above, above, "w_down", 2 * d + p, to_down),
                jnp.logical_and(z + d < planes, has_down),
            )

    w_y = copy(weight.at[their_rows], wh_at(z, y), "w_y", 0, to_y)

    def cols_x(q):
        return copy(
            cotangent.at[:, column(2 * mine[q] + xn)], cols_at(1, mine[q]), "cols_x", q, to_x
        )

    def cols_d(q):
        return copy(cols_at(1, mine[q]), cols_at(3, mine[q]), "cols_d", q, to_y)

    def cols_y(q):
        return copy(
            cotangent.at[:, column(2 * mine[q] + x)], cols_at(2, mine[q]), "cols_y", q, to_y
        )

    def cols_core(slab, name, q):
        ref = cols_at(slab, mine[q])
        return copy(ref, ref, name, q, to_core)

    def pass_x(q):
        arrive(cols_x(q))
        send(cols_d(q))
        send(cols_core(1, "cols_x_core", q))

    def pass_d(q):
        arrive(cols_d(q))
        send(cols_core(3, "cols_d_core", q))

    def pass_y(q):
        arrive(cols_y(q))
        send(cols_core(2, "cols_y_core", q))

    def lay_taps(j):
        tap_t[j, 0:span, :] = taps[:, lanes(j)]
        small[j] = jnp.zeros(small.shape[1:], f32)

    over(tiles, lay_taps)
    load_v.wait()
    load_g.wait()
    load_w.start()
    for made in load_c:
        made.start()

    def gate_tile(j):
        sig = jax.nn.sigmoid(gate_v[:, lanes(j)].astype(f32))
        got = (value_v[:, lanes(j)].astype(f32) * sig).astype(bf16).astype(f32)
        mixed[j, EDGE : EDGE + rows, :] = got
        edge_out[0, j] = mixed[j, rows : rows + EDGE, :].astype(bf16)
        edge_out[1, j] = mixed[j, EDGE : 2 * EDGE, :].astype(bf16)

    over(tiles, gate_tile)
    pl.semaphore_wait(barrier, len(peers))
    halo_prev = copy(edge_out.at[0], edge_in.at[0], "halo", 0, to_next)
    halo_next = copy(edge_out.at[1], edge_in.at[1], "halo", 1, to_prev)
    send(halo_prev, has_next)
    send(halo_next, has_prev)
    w_first(0, weight.at[my_rows], y)
    send(w_y)
    send(cols_y(0))
    for q in range(parts):
        send(cols_x(q))

    def fill(made, when, src, dst, at_row):
        @pl.when(when)
        def _():
            made.wait_recv()
            for j in range(tiles):
                dst[j, at_row : at_row + EDGE, :] = src[j].astype(f32)

        @pl.when(jnp.logical_not(when))
        def _():
            for j in range(tiles):
                dst[j, at_row : at_row + EDGE, :] = jnp.zeros((EDGE, LANES), f32)

    fill(halo_prev, has_prev, edge_in.at[0], mixed, 0)
    fill(halo_next, has_next, edge_in.at[1], mixed, EDGE + rows)

    def conv_tile(j):
        for r in range(0, rows, step):
            acc = tap_t[j, 0:1, :] * mixed[j, r + lead : r + lead + step, :]
            for k in range(1, span):
                at_row = r + k + lead
                acc = acc + tap_t[j, k : k + 1, :] * mixed[j, at_row : at_row + step, :]
            conv[j, r : r + step, :] = acc

    over(tiles, conv_tile)
    pass_x(0)
    for r in range(0, rows, step):
        at_rows = slice(r, r + step)
        total = conv[0, at_rows, :]
        for j in range(1, tiles):
            total = total + conv[j, at_rows, :]
        middle = jnp.sum(total, axis=1, keepdims=True) / width
        off = conv[0, at_rows, :] - middle
        square = off * off
        for j in range(1, tiles):
            off = conv[j, at_rows, :] - middle
            square = square + off * off
        stat_out[0, at_rows, :] = total
        stat_out[1, at_rows, :] = square
    stats = copy(stat_out.at[0:2], stat_in.at[0:2], "stats", 0, to_core)
    send(stats)
    arrive(w_y)
    w_first(1, wh_at(z, yn), yn)
    w_forward(1, 0)
    arrive(stats)
    for r in range(0, rows, step):
        at_rows = slice(r, r + step)
        here = jnp.sum(stat_out[0, at_rows, :], axis=1, keepdims=True)
        there = jnp.sum(stat_in[0, at_rows, :], axis=1, keepdims=True)
        both = stat_out[1, at_rows, :] + stat_in[1, at_rows, :]
        apart = (here - there) / width
        spread = jnp.sum(both, axis=1, keepdims=True) / (2 * width) + apart * apart / 4
        inv = lax.rsqrt(spread + 1e-06)
        rows_of[0, at_rows, :] = jnp.broadcast_to((here + there) / (2 * width), (step, LANES))
        rows_of[1, at_rows, :] = jnp.broadcast_to(inv, (step, LANES))

    def act_side(h):
        def act_tile(jj):
            j = h * tiles_side + jj
            normed = (conv[j] - rows_of[0]) * rows_of[1]
            pre = normed * gain[0:1, lanes(j)] + bias[0:1, lanes(j)]
            sig = jax.nn.sigmoid(pre)
            acts[h, :, lanes(jj)] = (pre * sig).astype(bf16)
            conv[j] = normed
            dact[j] = sig * (1.0 + pre * (1.0 - sig))

        over(tiles_side, act_tile)

    act_y = copy(acts.at[yn], acts.at[3], "act_y", 0, to_y)
    act_x = copy(acts.at[y], acts.at[2], "act_x", 0, to_x)
    act_d = copy(acts.at[3], acts.at[4], "act_d", 0, to_x)
    act_side(yn)
    send(act_y)
    act_side(y)
    send(act_x)
    for q in range(1, parts):
        pass_x(q)
        if q == 1:
            send(cols_y(1))
            w_forward(1, 1)
    for q in range(2, parts):
        send(cols_y(q))

    def factor_tile(j):
        sig = jax.nn.sigmoid(gate_v[:, lanes(j)].astype(f32))
        factor_v[j] = sig
        factor_g[j] = value_v[:, lanes(j)].astype(f32) * sig * (1.0 - sig)

    over(tiles, factor_tile)
    turned[0] = acts[y].T
    if planes > 2:
        w_forward(2, 0)
    arrive(act_y)
    send(act_d)
    pass_d(0)
    pass_y(0)
    if planes > 2:
        w_forward(2, 1)
    arrive(act_x)
    turned[1] = acts[2].T
    turned[2] = acts[3].T
    pass_d(1)
    pass_y(1)
    load_w.wait()
    for made in load_c:
        made.wait()

    def weight_of(zb):
        acc = jnp.dot(turned[0], cols[0, zb], preferred_element_type=f32)
        for slab in range(1, 4):
            acc = acc + jnp.dot(turned[slab], cols[slab, zb], preferred_element_type=f32)
        wg[2 * zb] = acc[:, 0:block]
        wg[2 * zb + 1] = acc[:, block : 2 * block]

    def up_copy(t, p):
        i = 2 * t + (yn if p == 0 else y)
        return copy(up_out.at[i], up_in.at[i], "up", 2 * t + p, to_up)

    def down_copy(t, p):
        i = 2 * t + (yn if p == 0 else y)
        return copy(down_out.at[i], down_in.at[i], "down", 2 * t + p, to_down)

    def fresh(m):
        for p in range(2):
            for t, made, out, when in (
                (planes - 1 - m, up_copy(planes - 1 - m, p), up_out, z == 0),
                (m, down_copy(m, p), down_out, z == planes - 1),
            ):
                i = 2 * t + (yn if p == 0 else y)

                @pl.when(when)
                def _():
                    out[i] = wg[i].astype(bf16)

                send(made, when)

    inner = jnp.logical_and(has_up, has_down)
    lower = jnp.logical_and(inner, 2 * z < planes)
    upper = jnp.logical_and(inner, 2 * z >= planes)

    def relay(n, going_up, side_of):
        m, p = n // 2, n % 2
        t = planes - 1 - m if going_up else m
        if not 0 <= m < planes - 1:
            return
        i = 2 * t + (yn if p == 0 else y)
        made = up_copy(t, p) if going_up else down_copy(t, p)
        out, got = (up_out, up_in) if going_up else (down_out, down_in)
        when = jnp.logical_and(side_of, z < t if going_up else z > t)

        @pl.when(when)
        def _():
            made.wait_recv()
            out[i] = (wg[i] + got[i].astype(f32)).astype(bf16)

        send(made, when)

    def serve(n):
        relay(n, True, lower)
        relay(n - 1, False, lower)
        relay(n, False, upper)
        relay(n - 1, True, upper)

    arrive(cols_core(3, "cols_d_core", 0))
    arrive(cols_core(3, "cols_d_core", 1))
    arrive(cols_core(1, "cols_x_core", 0))
    arrive(cols_core(1, "cols_x_core", 1))
    arrive(cols_core(2, "cols_y_core", 0))
    arrive(cols_core(2, "cols_y_core", 1))
    arrive(act_d)
    turned[3] = acts[4].T
    early = parts // 4
    for zb in range(early):
        weight_of(zb)
        weight_of(planes - 1 - zb)
        fresh(zb)
    for d in range(3, planes):
        w_forward(d, 0)
    for q in range(2, parts):
        pass_d(q)
    for d in range(3, planes):
        w_forward(d, 1)

    def product(slab):
        acc = None
        for zb in range(planes):
            got = lax.dot_general(
                cols[slab, zb], wh[zb], (((1,), (1,)), ((), ())), preferred_element_type=f32
            )
            acc = got if acc is None else acc + got
        return acc

    part_x = [
        [copy(part_out.at[n, h], part_in.at[n, h], "part_x", 2 * n + h, to_x) for h in range(2)]
        for n in range(2)
    ]
    cut = side // 2

    def partial(slab, n):
        got = product(slab)
        for h in range(2):
            part_out[n, h] = got[:, h * cut : (h + 1) * cut].astype(bf16)
            send(part_x[n][h])

    for q in range(2, parts):
        arrive(cols_core(3, "cols_d_core", q))
    partial(3, 1)
    for q in range(2, parts):
        arrive(cols_core(1, "cols_x_core", q))
    partial(1, 0)
    part[0] = product(0)
    for q in range(2, parts):
        pass_y(q)
        if q == 2:
            serve(0)
    for q in range(2, parts):
        arrive(cols_core(2, "cols_y_core", q))
    part[1] = product(2)
    part_y = [copy(half_out.at[h], half_in.at[h], "part_y", h, to_y) for h in range(2)]

    def fold(h):
        arrive(part_x[1][h])
        got = part[1, :, h * cut : (h + 1) * cut] + part_in[1, h].astype(f32)
        half_out[h] = got.astype(bf16)
        send(part_y[h])

    fold(0)
    for zb in range(early, planes // 2):
        weight_of(planes - 1 - zb)
        weight_of(zb)
        fresh(zb)
    for m in range(planes // 2, planes - 1):
        fresh(m)
    fold(1)
    serve(1)
    stat_out[2] = jnp.zeros((rows, LANES), f32)
    stat_out[3] = jnp.zeros((rows, LANES), f32)

    def back_tile(j, got):
        pre_grad = got * dact[j]
        normed = conv[j]
        scaled = pre_grad * gain[0:1, lanes(j)]
        crossed = pre_grad * normed
        dact[j] = scaled
        stat_out[2] = stat_out[2] + scaled
        stat_out[3] = stat_out[3] + scaled * normed
        small[j, span : span + 1, :] = jnp.sum(crossed, axis=0, keepdims=True)
        small[j, span + 1 : span + 2, :] = jnp.sum(pre_grad, axis=0, keepdims=True)

    tiles_cut = tiles_side // 2

    def back_mine(h):
        arrive(part_x[0][h])

        def one(jj):
            at_side = lanes(h * tiles_cut + jj)
            got = part[0, :, at_side] + part_in[0, h, :, lanes(jj)].astype(f32)
            back_tile(y * tiles_side + h * tiles_cut + jj, got)

        over(tiles_cut, one)

    def back_theirs(h):
        arrive(part_y[h])

        def one(jj):
            back_tile(yn * tiles_side + h * tiles_cut + jj, half_in[h, :, lanes(jj)].astype(f32))

        over(tiles_cut, one)

    back_mine(0)
    back_theirs(0)
    back_mine(1)
    back_theirs(1)
    norm = copy(stat_out.at[2:4], stat_in.at[2:4], "norm", 0, to_core)
    send(norm)
    arrive(norm)
    for r in range(0, rows, step):
        at_rows = slice(r, r + step)
        for n in range(2):
            both = stat_out[2 + n, at_rows, :] + stat_in[2 + n, at_rows, :]
            got = jnp.sum(both, axis=1, keepdims=True) / (2 * width)
            rows_of[2 + n, at_rows, :] = jnp.broadcast_to(got, (step, LANES))

    def grad_tile(j):
        grads[j, EDGE : EDGE + rows, :] = rows_of[1] * (
            dact[j] - rows_of[2] - conv[j] * rows_of[3]
        )
        gedge_out[0, j] = grads[j, rows : rows + EDGE, :]
        gedge_out[1, j] = grads[j, EDGE : 2 * EDGE, :]

    over(tiles, grad_tile)
    grad_prev = copy(gedge_out.at[0], gedge_in.at[0], "grad_halo", 0, to_next)
    grad_next = copy(gedge_out.at[1], gedge_in.at[1], "grad_halo", 1, to_prev)
    send(grad_prev, has_next)
    send(grad_next, has_prev)
    serve(2)

    def tap_tile(j):
        def block_of(r, acc):
            base = pl.multiple_of(r * step, 8)
            own = grads[j, pl.ds(base + EDGE, step), :]
            out = []
            for k in range(span):
                got = own * mixed[j, pl.ds(base + k + lead, step), :]
                out.append(acc[k] + jnp.sum(got.reshape(step // 8, 8, LANES), axis=0))
            return tuple(out)

        start = tuple(jnp.zeros((8, LANES), f32) for _ in range(span))
        acc = lax.fori_loop(0, rows // step, block_of, start)
        for k in range(span):
            small[j, k : k + 1, :] = jnp.sum(acc[k], axis=0, keepdims=True)

    over(tiles, tap_tile)
    place = 2 * y + x
    near = [(to_x, 2 * y + xn), (to_y, 2 * yn + x), (to_d, 2 * yn + xn)]
    own_tiles = pl.ds(place * quarter, quarter)
    gather = [
        copy(small.at[pl.ds(p * quarter, quarter)], plane_in.at[n], "plane_in", n, dev)
        for n, (dev, p) in enumerate(near)
    ]
    for made in gather:
        send(made)
    fill(grad_prev, has_prev, gedge_in.at[0], grads, 0)
    fill(grad_next, has_next, gedge_in.at[1], grads, EDGE + rows)

    def mixed_tile(j):
        for r in range(0, rows, step):
            at_row = r + EDGE + half
            acc = tap_t[j, 0:1, :] * grads[j, at_row : at_row + step, :]
            for k in range(1, span):
                at_row = r + EDGE + half - k
                acc = acc + tap_t[j, k : k + 1, :] * grads[j, at_row : at_row + step, :]
            tile[r : r + step, :] = acc
        got = tile[...]
        value_v[:, lanes(j)] = (got * factor_v[j]).astype(bf16)
        gate_v[:, lanes(j)] = (got * factor_g[j]).astype(bf16)

    def mixed_tiles(lo, hi):
        lax.fori_loop(lo, hi, lambda j, c: (mixed_tile(j), c)[1], 0)

    mixed_tiles(0, tiles_side)
    for made in gather:
        arrive(made)
    across[z] = small[own_tiles] + plane_in[0] + plane_in[1] + plane_in[2]
    for d in range(1, planes):
        made = copy(across.at[z], across.at[z], "across", d, at(lax.rem(z + d, planes), y, x))
        send(made)
    for n in range(3, 2 * planes - 1):
        serve(n)
    mixed_tiles(tiles_side, tiles)
    store_v = pltpu.make_async_copy(value_v, value_grad, local_sem.at[0])
    store_g = pltpu.make_async_copy(gate_v, gate_grad, local_sem.at[1])
    store_v.start()
    store_g.start()

    def finish(p):
        i = 2 * z + (yn if p == 0 else y)
        for t in range(planes):

            @pl.when(z == t)
            def _():
                total = wg[i]
                if t > 0:
                    up_copy(t, p).wait_recv()
                    total = total + up_in[i].astype(f32)
                if t < planes - 1:
                    down_copy(t, p).wait_recv()
                    total = total + down_in[i].astype(f32)
                if p == 0:
                    back_out[...] = total.astype(bf16)
                else:
                    weight_v[0] = total

    def across_out():
        for d in range(1, planes):
            arrive(copy(across.at[z], across.at[z], "across", d, to_core))
        total = across[0]
        for d in range(1, planes):
            total = total + across[d]
        owned[...] = total
        small_all[own_tiles] = total
        for made in spread_out:
            send(made)

    spread_out = [
        copy(owned, small_all.at[own_tiles], "plane_out", n, dev) for n, (dev, p) in enumerate(near)
    ]
    finish(0)
    back = copy(back_out, back_in, "w_back", 0, to_y)
    send(back)
    across_out()
    finish(1)
    store_w = pltpu.make_async_copy(weight_v.at[0], weight_grad.at[my_rows], local_sem.at[2])
    store_w.start()
    for made in spread_out:
        arrive(made)
    for j in range(tiles):
        at_lanes = slice(j * LANES, (j + 1) * LANES)
        tap_grad[:, at_lanes] = small_all[j, 0:span, :]
        gain_grad[:, at_lanes] = small_all[j, span : span + 1, :]
        bias_grad[:, at_lanes] = small_all[j, span + 1 : span + 2, :]
    arrive(back)
    weight_v[1] = back_in[...].astype(f32)
    store_t = pltpu.make_async_copy(weight_v.at[1], weight_grad.at[their_rows], local_sem.at[3])
    store_t.start()
    for made, when in pending:
        if when is None:
            made.wait_send()
        else:
            pl.when(when)(made.wait_send)
    for made in (store_v, store_g, store_w, store_t):
        made.wait()


def fused_on_device(value_in, gate_in, taps, norm_gain, norm_bias, proj_weight, out_grad):
    f32, bf16 = jnp.float32, jnp.bfloat16
    rows, width = value_in.shape
    span = taps.shape[0]
    block = proj_weight.shape[1]
    planes = lax.axis_size("sp") // 4
    blocks = 2 * planes
    side = width // 2
    tiles = width // LANES
    step = max(n for n in (8, 16, 24, 32, 40) if rows % n == 0)
    kept = -(-(span + 2) // 8) * 8
    first, total = slot_table(planes, blocks)
    vmem, dma = pltpu.VMEM, pltpu.SemaphoreType.DMA
    scratch = [
        vmem((rows, width), bf16),
        vmem((rows, width), bf16),
        vmem((4, planes, rows, 2 * block), bf16),
        vmem((planes, side, 2 * block), bf16),
        vmem((tiles, kept, LANES), f32),
        vmem((tiles, rows + 2 * EDGE, LANES), f32),
        vmem((2, tiles, EDGE, LANES), bf16),
        vmem((2, tiles, EDGE, LANES), bf16),
        vmem((tiles, rows, LANES), f32),
        vmem((tiles, rows, LANES), f32),
        vmem((4, rows, LANES), f32),
        vmem((4, rows, LANES), f32),
        vmem((4, rows, LANES), f32),
        vmem((5, rows, side), bf16),
        vmem((tiles, rows, LANES), f32),
        vmem((tiles, rows, LANES), f32),
        vmem((2, rows, side), f32),
        vmem((2, 2, rows, side // 2), bf16),
        vmem((2, 2, rows, side // 2), bf16),
        vmem((2, rows, side // 2), bf16),
        vmem((2, rows, side // 2), bf16),
        vmem((blocks, side, block), f32),
        vmem((blocks, side, block), bf16),
        vmem((blocks, side, block), bf16),
        vmem((blocks, side, block), bf16),
        vmem((blocks, side, block), bf16),
        vmem((side, block), bf16),
        vmem((side, block), bf16),
        vmem((2, side, block), f32),
        vmem((4, side, rows), bf16),
        vmem((tiles, rows + 2 * EDGE, LANES), f32),
        vmem((2, tiles, EDGE, LANES), f32),
        vmem((2, tiles, EDGE, LANES), f32),
        vmem((tiles, kept, LANES), f32),
        vmem((3, tiles // 4, kept, LANES), f32),
        vmem((planes, tiles // 4, kept, LANES), f32),
        vmem((tiles // 4, kept, LANES), f32),
        vmem((tiles, kept, LANES), f32),
        vmem((rows, LANES), f32),
        dma((total,)),
        dma((total,)),
        dma((3 + blocks,)),
    ]
    whole, hbm = pl.BlockSpec(memory_space=pltpu.VMEM), pl.BlockSpec(memory_space=pl.ANY)
    outs = pl.pallas_call(
        functools.partial(kernel, (rows, width, span, planes, block, step), first),
        out_shape=(
            jax.ShapeDtypeStruct((rows, width), bf16),
            jax.ShapeDtypeStruct((rows, width), bf16),
            jax.ShapeDtypeStruct((span, width), f32),
            jax.ShapeDtypeStruct((1, width), f32),
            jax.ShapeDtypeStruct((1, width), f32),
            jax.ShapeDtypeStruct((width, block), f32),
        ),
        in_specs=[hbm, hbm, whole, whole, whole, hbm, hbm],
        out_specs=[hbm, hbm, whole, whole, whole, hbm],
        scratch_shapes=scratch,
        compiler_params=pltpu.CompilerParams(
            collective_id=0, has_side_effects=True, vmem_limit_bytes=62 * 2**20
        ),
    )(
        value_in,
        gate_in,
        taps,
        norm_gain.reshape(1, width),
        norm_bias.reshape(1, width),
        proj_weight,
        out_grad,
    )
    value_grad, gate_grad, tap_grad, gain_grad, bias_grad, weight_grad = outs
    return (
        value_grad,
        gate_grad,
        tap_grad,
        gain_grad.reshape(width),
        bias_grad.reshape(width),
        weight_grad,
    )


def solution(mesh):
    fused = mesh.shape["tp"] == 2 and mesh.shape["sp"] % 4 == 0
    return jax.shard_map(
        fused_on_device if fused else on_device,
        mesh=mesh,
        in_specs=(
            P("sp", "tp"),
            P("sp", "tp"),
            P(None, "tp"),
            P("tp"),
            P("tp"),
            P("tp", "sp"),
            P("sp", None),
        ),
        out_specs=(P("sp", "tp"), P("sp", "tp"), P(None, "tp"), P("tp"), P("tp"), P("tp", "sp")),
        check_vma=False,
    )
```

```python
import functools
import jax
import jax.numpy as jnp
from jax import lax
from jax.experimental import pallas as pl
from jax.experimental.pallas import tpu as pltpu
from jax.sharding import PartitionSpec as P


def padded_rows(cells, width):
    count = lax.axis_size("sp")
    ends = count - 1
    rows = cells.shape[0]
    before = lax.ppermute(cells[rows - width :], "sp", [(i, i + 1) for i in range(ends)])
    after = lax.ppermute(cells[:width], "sp", [(i + 1, i) for i in range(ends)])
    return jnp.concatenate([before, cells, after], axis=0)


def on_device(*arrays):
    return compute(*arrays)


def compute(value_in, gate_in, taps, norm_gain, norm_bias, proj_weight, out_grad):
    f32, bf16 = jnp.float32, jnp.bfloat16
    rows, local_width = value_in.shape
    span = taps.shape[0]
    half = span // 2
    tp = lax.axis_size("tp")
    count = lax.axis_size("sp")
    inner = 1 << ((count.bit_length() - 1) // 2)
    outer = count // inner
    width_all = local_width * tp
    block = proj_weight.shape[1]
    me = lax.axis_index("sp")
    plane, place = me // inner, me % inner
    core = lax.axis_index("tp")

    def swap(array, d):
        return lax.ppermute(
            array, "sp", [(i, i - i % inner + ((i % inner) ^ d)) for i in range(count)]
        )

    def shift(array, e):
        return lax.ppermute(array, "sp", [(i, (i + e * inner) % count) for i in range(count)])

    def across(array, t):
        return lax.ppermute(array, "tp", [(c, c ^ t) for c in range(tp)])

    def tp_sum(array):
        return array + sum(across(array, t) for t in range(1, tp))

    gate_sig = jax.nn.sigmoid(gate_in.astype(f32))
    value_f = value_in.astype(f32)
    mixed = (value_f * gate_sig).astype(bf16)
    padded = padded_rows(mixed, half).astype(f32)

    def columns_of(where, first, blocks):
        return jnp.concatenate(
            [
                lax.dynamic_slice_in_dim(
                    out_grad,
                    (((plane + first + e) % outer) * inner + where) * block,
                    block,
                    axis=1,
                )
                for e in range(blocks)
            ],
            axis=1,
        )

    share = outer // tp
    own_columns = columns_of(place, 0, outer)
    arrived = [swap(columns_of(place ^ d, core * share, share), d) for d in range(1, inner)]
    weights = [proj_weight] + [shift(proj_weight, -e) for e in range(1, outer)]
    weight_cols = jnp.concatenate(weights, axis=1)
    cotangents = [own_columns]
    for got in arrived:
        parts = jnp.stack([got] + [across(got, t) for t in range(1, tp)])
        cotangents.append(
            jnp.concatenate(
                [
                    lax.dynamic_index_in_dim(parts, core ^ j, axis=0, keepdims=False)
                    for j in range(tp)
                ],
                axis=1,
            )
        )

    conv = jnp.zeros((rows, local_width), f32)
    for k in range(span):
        conv = conv + taps[k] * padded[k : k + rows]
    mean = tp_sum(jnp.sum(conv, axis=1)) / width_all
    centred = conv - mean[:, None]
    spread = tp_sum(jnp.sum(centred * centred, axis=1)) / width_all
    inv = lax.rsqrt(spread + 1e-06)
    normed = centred * inv[:, None]
    pre = normed * norm_gain + norm_bias
    sig_pre = jax.nn.sigmoid(pre)
    act = (pre * sig_pre).astype(bf16)
    acts = [act] + [swap(act, d) for d in range(1, inner)]

    partial = [
        lax.dot_general(c, weight_cols, (((1,), (1,)), ((), ())), preferred_element_type=f32)
        for c in cotangents
    ]
    act_grad = partial[0]
    sending = lax.optimization_barrier(([p.astype(bf16) for p in partial[1:]], acts))[0]
    for d in range(1, inner):
        got = swap(sending[d - 1], d)
        act_grad = act_grad + got.astype(f32)

    pre_grad = act_grad * sig_pre * (1.0 + pre * (1.0 - sig_pre))
    normed_grad = pre_grad * norm_gain
    sums = tp_sum(
        jnp.stack([jnp.sum(normed_grad, axis=1), jnp.sum(normed_grad * normed, axis=1)])
    )
    first, second = sums[0], sums[1]
    conv_grad = inv[:, None] * (
        normed_grad - first[:, None] / width_all - normed * second[:, None] / width_all
    )
    extended = lax.optimization_barrier(padded_rows(conv_grad, half))
    tap_local = jnp.stack([jnp.sum(conv_grad * padded[k : k + rows], axis=0) for k in range(span)])
    gain_local = jnp.sum(pre_grad * normed, axis=0)
    bias_local = jnp.sum(pre_grad, axis=0)
    small = jnp.concatenate([tap_local, gain_local[None], bias_local[None]], axis=0)
    small = small + sum(swap(small, d) for d in range(1, inner))
    small = small + sum(shift(small, e) for e in range(1, outer))
    tap_grad, gain_grad, bias_grad = small[:span], small[span], small[span + 1]

    mixed_grad = jnp.zeros((rows, local_width), f32)
    for k in range(span):
        mixed_grad = mixed_grad + taps[k] * extended[2 * half - k : 2 * half - k + rows]
    value_grad = (mixed_grad * gate_sig).astype(bf16)
    gate_grad = (mixed_grad * value_f * gate_sig * (1.0 - gate_sig)).astype(bf16)

    weight_part = lax.dot_general(
        jnp.concatenate(acts, axis=0),
        jnp.concatenate(cotangents, axis=0),
        (((0,), (0,)), ((), ())),
        preferred_element_type=f32,
    )
    weight_grad = weight_part[:, :block]
    for e in range(1, outer):
        sent = weight_part[:, e * block : (e + 1) * block].astype(bf16)
        got = shift(sent, e)
        weight_grad = weight_grad + got.astype(f32)
    return (value_grad, gate_grad, tap_grad, gain_grad, bias_grad, weight_grad)


LANES = 128
EDGE = 16
GROUP = 16
MESH = pl.DeviceIdType.MESH


def slot_table(planes, blocks):
    parts = blocks // 2
    sizes = {
        "halo": 4,
        "cols_x": parts,
        "cols_x_core": parts,
        "cols_d": parts,
        "cols_d_core": parts,
        "cols_y": parts,
        "cols_y_core": parts,
        "w_y": 1,
        "w_up": 2 * (planes - 1),
        "w_down": 2 * (planes - 1),
        "stats": 1,
        "act_x": 1,
        "act_y": 1,
        "act_d": 1,
        "part_x": 4,
        "part_y": 2,
        "up": blocks,
        "down": blocks,
        "w_back": 1,
        "norm": 1,
        "grad_halo": 2,
        "plane_in": 3,
        "across": planes,
        "plane_out": 3,
    }
    first, total = {}, 0
    for name, size in sizes.items():
        first[name] = total
        total += size
    return first, total


def kernel(
    shape,
    first,
    value,
    gate,
    taps_hbm,
    gain_hbm,
    bias_hbm,
    weight,
    cotangent,
    value_grad,
    gate_grad,
    small_grad,
    weight_mine,
    weight_back,
    value_v,
    gate_v,
    taps,
    gain,
    bias,
    cols,
    wh,
    tap_t,
    mixed,
    edge_in,
    conv,
    dact,
    stat_out,
    stat_in,
    rows_of,
    acts,
    factor_v,
    factor_g,
    part,
    part_out,
    part_in,
    half_out,
    half_in,
    wg,
    up_out,
    down_out,
    up_in,
    down_in,
    back_out,
    back_in,
    weight_v,
    turned,
    grads,
    gedge_out,
    gedge_in,
    small,
    plane_in,
    across,
    owned,
    small_all,
    tile,
    send_sem,
    recv_sem,
    local_sem,
):
    rows, width, span, planes, block, step = shape
    f32, bf16 = jnp.float32, jnp.bfloat16
    blocks = 2 * planes
    parts = blocks // 2
    side = width // 2
    tiles = width // LANES
    tiles_side = tiles // 2
    quarter = tiles // 4
    count = 4 * planes
    half = span // 2
    lead = EDGE - half

    me, core = lax.axis_index("sp"), lax.axis_index("tp")
    z, y, x = lax.div(me, 4), lax.rem(lax.div(me, 2), 2), lax.rem(me, 2)
    yn, xn = 1 - y, 1 - x

    def at(zz, yy, xx):
        return (zz * 4 + yy * 2 + xx, core)

    to_x, to_y, to_d = at(z, y, xn), at(z, yn, x), at(z, yn, xn)
    to_core = (me, 1 - core)
    to_up, to_down = (me + 4, core), (me - 4, core)
    to_next, to_prev = (me + 1, core), (me - 1, core)
    has_up, has_down = z < planes - 1, z > 0
    has_next, has_prev = me < count - 1, me > 0

    pending = []

    def copy(src, dst, name, index, device):
        at_slot = first[name] + index
        return pltpu.make_async_remote_copy(
            src_ref=src,
            dst_ref=dst,
            send_sem=send_sem.at[at_slot],
            recv_sem=recv_sem.at[at_slot],
            device_id=device,
            device_id_type=MESH,
        )

    def send(made, when=None):
        pending.append((made, when))
        if when is None:
            made.start()
        else:
            pl.when(when)(made.start)

    def arrive(made, when=None):
        if when is None:
            made.wait_recv()
        else:
            pl.when(when)(made.wait_recv)

    def lanes(j):
        return pl.ds(pl.multiple_of(j * LANES, LANES), LANES)

    def over(n, body):
        def step_of(j, carry):
            body(j)
            return carry

        lax.fori_loop(0, n, step_of, 0)

    my_rows = pl.ds(pl.multiple_of(y * side, side), side)
    their_rows = pl.ds(pl.multiple_of(yn * side, side), side)

    def column(b):
        return pl.ds(pl.multiple_of(b * block, block), block)

    low = 2 * z < planes
    turn = []
    for q in range(planes - 1):
        down_to = planes - 1 - q
        fall = down_to - jnp.where(down_to <= z, 1, 0)
        rise = q + jnp.where(q >= z, 1, 0)
        turn.append(jnp.where(low, fall, rise))
    turn.append(z)
    mine = [2 * zb + core for zb in turn]

    def cols_at(slab, i):
        return cols.at[slab, lax.div(i, 2), :, column(lax.rem(i, 2))]

    def wh_at(zz, yy):
        return wh.at[zz, :, column(yy)]

    load_v = pltpu.make_async_copy(value, value_v, local_sem.at[0])
    load_g = pltpu.make_async_copy(gate, gate_v, local_sem.at[1])
    load_w = pltpu.make_async_copy(weight.at[my_rows], wh_at(z, y), local_sem.at[2])
    load_c = [
        pltpu.make_async_copy(
            cotangent.at[:, column(2 * i + x)],
            cols.at[0, i // 2, :, (i % 2) * block : (i % 2 + 1) * block],
            local_sem.at[3 + i],
        )
        for i in range(blocks)
    ]
    load_s = [
        pltpu.make_async_copy(src, dst, local_sem.at[3 + blocks + n])
        for n, (src, dst) in enumerate(((taps_hbm, taps), (gain_hbm, gain), (bias_hbm, bias)))
    ]

    barrier = pltpu.get_barrier_semaphore()
    peers = [to_x, to_y, to_d, to_core]
    peers += [at(lax.rem(z + d, planes), y, x) for d in range(1, planes)]
    peers += [(lax.rem(me + 1, count), core), (lax.rem(me + count - 1, count), core)]
    for peer in peers:
        pl.semaphore_signal(barrier, inc=1, device_id=peer, device_id_type=MESH)
    load_v.start()
    load_g.start()
    for made in load_s:
        made.start()

    def w_copies(d, p):
        yb = y if p == 0 else yn
        index = 2 * (d - 1) + p
        below = wh_at(lax.rem(z - d + planes, planes), yb)
        above = wh_at(lax.rem(z + d, planes), yb)
        return (
            copy(below, below, "w_up", index, to_up),
            copy(above, above, "w_down", index, to_down),
        )

    def w_first(p, src, yb):
        dst = wh_at(z, yb)
        send(copy(src, dst, "w_up", p, to_up), has_up)
        send(copy(src, dst, "w_down", p, to_down), has_down)

    def w_forward(d, p):
        up, down = w_copies(d, p)
        yb = y if p == 0 else yn
        below = wh_at(lax.rem(z - d + planes, planes), yb)
        above = wh_at(lax.rem(z + d, planes), yb)
        arrive(up, z >= d)
        if d < planes - 1:
            send(copy(below, below, "w_up", 2 * d + p, to_up), jnp.logical_and(z >= d, has_up))
        arrive(down, z + d < planes)
        if d < planes - 1:
            send(
                copy(above, above, "w_down", 2 * d + p, to_down),
                jnp.logical_and(z + d < planes, has_down),
            )

    w_y = copy(weight.at[their_rows], wh_at(z, y), "w_y", 0, to_y)

    def cols_x(q):
        return copy(
            cotangent.at[:, column(2 * mine[q] + xn)], cols_at(1, mine[q]), "cols_x", q, to_x
        )

    def cols_d(q):
        return copy(cols_at(1, mine[q]), cols_at(3, mine[q]), "cols_d", q, to_y)

    def cols_y(q):
        return copy(
            cotangent.at[:, column(2 * mine[q] + x)], cols_at(2, mine[q]), "cols_y", q, to_y
        )

    def cols_core(slab, name, q):
        ref = cols_at(slab, mine[q])
        return copy(ref, ref, name, q, to_core)

    def pass_x(q):
        arrive(cols_x(q))
        send(cols_d(q))
        send(cols_core(1, "cols_x_core", q))

    def pass_d(q):
        arrive(cols_d(q))
        send(cols_core(3, "cols_d_core", q))

    def pass_y(q):
        arrive(cols_y(q))
        send(cols_core(2, "cols_y_core", q))

    pl.semaphore_wait(barrier, len(peers))
    halo = []
    for n, (src, near_rows) in enumerate(
        ((value, rows - EDGE), (gate, rows - EDGE), (value, 0), (gate, 0))
    ):
        made = copy(
            src.at[near_rows : near_rows + EDGE],
            edge_in.at[n],
            "halo",
            n,
            to_next if n < 2 else to_prev,
        )
        send(made, has_next if n < 2 else has_prev)
        halo.append(made)
    w_first(0, weight.at[my_rows], y)
    send(w_y)
    send(cols_y(0))
    for q in range(parts):
        send(cols_x(q))
    load_w.start()
    for made in load_c:
        made.start()
    for made in load_s:
        made.wait()
    load_v.wait()
    load_g.wait()

    def gate_tile(j):
        tap_t[j, 0:span, :] = taps[:, lanes(j)]
        small[j] = jnp.zeros(small.shape[1:], f32)
        sig = jax.nn.sigmoid(gate_v[:, lanes(j)].astype(f32))
        got = (value_v[:, lanes(j)].astype(f32) * sig).astype(bf16).astype(f32)
        mixed[j, EDGE : EDGE + rows, :] = got

    over(tiles, gate_tile)

    def fill(made, when, src, dst, at_row):
        @pl.when(when)
        def _():
            made.wait_recv()
            for j in range(tiles):
                dst[j, at_row : at_row + EDGE, :] = src[j].astype(f32)

        @pl.when(jnp.logical_not(when))
        def _():
            for j in range(tiles):
                dst[j, at_row : at_row + EDGE, :] = jnp.zeros((EDGE, LANES), f32)

    def fill_mixed(first_of, when, at_row):
        @pl.when(when)
        def _():
            halo[first_of].wait_recv()
            halo[first_of + 1].wait_recv()
            for j in range(tiles):
                at_lanes = slice(j * LANES, (j + 1) * LANES)
                sig = jax.nn.sigmoid(edge_in[first_of + 1, :, at_lanes].astype(f32))
                got = edge_in[first_of, :, at_lanes].astype(f32) * sig
                mixed[j, at_row : at_row + EDGE, :] = got.astype(bf16).astype(f32)

        @pl.when(jnp.logical_not(when))
        def _():
            for j in range(tiles):
                mixed[j, at_row : at_row + EDGE, :] = jnp.zeros((EDGE, LANES), f32)

    fill_mixed(0, has_prev, 0)
    fill_mixed(2, has_next, EDGE + rows)

    def conv_tile(j):
        for r in range(0, rows, step):
            acc = tap_t[j, 0:1, :] * mixed[j, r + lead : r + lead + step, :]
            for k in range(1, span):
                at_row = r + k + lead
                acc = acc + tap_t[j, k : k + 1, :] * mixed[j, at_row : at_row + step, :]
            conv[j, r : r + step, :] = acc

    over(tiles, conv_tile)
    for r in range(0, rows, step):
        at_rows = slice(r, r + step)
        total = conv[0, at_rows, :]
        for j in range(1, tiles):
            total = total + conv[j, at_rows, :]
        middle = jnp.sum(total, axis=1, keepdims=True) / width
        off = conv[0, at_rows, :] - middle
        square = off * off
        for j in range(1, tiles):
            off = conv[j, at_rows, :] - middle
            square = square + off * off
        stat_out[0, at_rows, :] = total
        stat_out[1, at_rows, :] = square
    stats = copy(stat_out.at[0:2], stat_in.at[0:2], "stats", 0, to_core)
    send(stats)
    arrive(w_y)
    w_first(1, wh_at(z, yn), yn)
    w_forward(1, 0)
    arrive(stats)
    for r in range(0, rows, step):
        at_rows = slice(r, r + step)
        here = jnp.sum(stat_out[0, at_rows, :], axis=1, keepdims=True)
        there = jnp.sum(stat_in[0, at_rows, :], axis=1, keepdims=True)
        both = stat_out[1, at_rows, :] + stat_in[1, at_rows, :]
        apart = (here - there) / width
        spread = jnp.sum(both, axis=1, keepdims=True) / (2 * width) + apart * apart / 4
        inv = lax.rsqrt(spread + 1e-06)
        rows_of[0, at_rows, :] = jnp.broadcast_to((here + there) / (2 * width), (step, LANES))
        rows_of[1, at_rows, :] = jnp.broadcast_to(inv, (step, LANES))

    def act_side(h):
        def act_tile(jj):
            j = h * tiles_side + jj
            normed = (conv[j] - rows_of[0]) * rows_of[1]
            pre = normed * gain[0:1, lanes(j)] + bias[0:1, lanes(j)]
            sig = jax.nn.sigmoid(pre)
            acts[h, :, lanes(jj)] = (pre * sig).astype(bf16)
            conv[j] = normed
            dact[j] = sig * (1.0 + pre * (1.0 - sig))

        over(tiles_side, act_tile)

    act_y = copy(acts.at[yn], acts.at[3], "act_y", 0, to_y)
    act_x = copy(acts.at[y], acts.at[2], "act_x", 0, to_x)
    act_d = copy(acts.at[3], acts.at[4], "act_d", 0, to_x)
    act_side(yn)
    send(act_y)
    act_side(y)
    send(act_x)
    pass_x(0)
    pass_x(1)
    pass_y(0)
    for q in range(2, parts - 1):
        pass_x(q)
    w_forward(1, 1)
    pass_x(parts - 1)
    for q in range(1, parts):
        send(cols_y(q))

    def factor_tile(j):
        sig = jax.nn.sigmoid(gate_v[:, lanes(j)].astype(f32))
        factor_v[j] = sig
        factor_g[j] = value_v[:, lanes(j)].astype(f32) * sig * (1.0 - sig)

    over(tiles, factor_tile)
    turned[0] = acts[y].T
    arrive(act_y)
    send(act_d)
    if planes > 2:
        w_forward(2, 0)
    arrive(act_x)
    turned[1] = acts[2].T
    turned[2] = acts[3].T
    pass_d(0)
    if planes > 2:
        w_forward(2, 1)
    pass_d(1)
    load_w.wait()
    for made in load_c:
        made.wait()

    def weight_of(zb):
        acc = jnp.dot(turned[0], cols[0, zb], preferred_element_type=f32)
        for slab in range(1, 4):
            acc = acc + jnp.dot(turned[slab], cols[slab, zb], preferred_element_type=f32)
        wg[2 * zb] = acc[:, 0:block]
        wg[2 * zb + 1] = acc[:, block : 2 * block]

    def up_copy(t, p):
        i = 2 * t + (yn if p == 0 else y)
        return copy(up_out.at[i], up_in.at[i], "up", 2 * t + p, to_up)

    def down_copy(t, p):
        i = 2 * t + (yn if p == 0 else y)
        return copy(down_out.at[i], down_in.at[i], "down", 2 * t + p, to_down)

    def fresh(m, p):
        for t, made, out, when in (
            (planes - 1 - m, up_copy(planes - 1 - m, p), up_out, z == 0),
            (m, down_copy(m, p), down_out, z == planes - 1),
        ):
            i = 2 * t + (yn if p == 0 else y)

            @pl.when(when)
            def _():
                out[i] = wg[i].astype(bf16)

            send(made, when)

    def finish(p):
        i = 2 * z + (yn if p == 0 else y)
        for t in range(planes):

            @pl.when(z == t)
            def _():
                total = wg[i]
                if t > 0:
                    up_copy(t, p).wait_recv()
                    total = total + up_in[i].astype(f32)
                if t < planes - 1:
                    down_copy(t, p).wait_recv()
                    total = total + down_in[i].astype(f32)
                if p == 0:
                    back_out[...] = total.astype(bf16)
                else:
                    weight_v[...] = total

    back = copy(back_out, back_in, "w_back", 0, to_y)
    inner = jnp.logical_and(has_up, has_down)
    lower = jnp.logical_and(inner, 2 * z < planes)
    upper = jnp.logical_and(inner, 2 * z >= planes)

    def relay(n, going_up, side_of):
        m, p = n // 2, n % 2
        t = planes - 1 - m if going_up else m
        if not 0 <= m < planes - 1:
            return
        i = 2 * t + (yn if p == 0 else y)
        made = up_copy(t, p) if going_up else down_copy(t, p)
        out, got = (up_out, up_in) if going_up else (down_out, down_in)
        when = jnp.logical_and(side_of, z < t if going_up else z > t)

        @pl.when(when)
        def _():
            made.wait_recv()
            out[i] = (wg[i] + got[i].astype(f32)).astype(bf16)

        send(made, when)

    def serve_near(n):
        relay(n, True, lower)
        relay(n, False, upper)

    def serve_far(n):
        relay(n, False, lower)
        relay(n, True, upper)

    def weigh(q):
        arrive(cols_core(1, "cols_x_core", q))
        arrive(cols_core(3, "cols_d_core", q))
        arrive(cols_core(2, "cols_y_core", q))
        weight_of(turn[q])

    arrive(act_d)
    turned[3] = acts[4].T
    weigh(0)
    fresh(0, 0)
    fresh(0, 1)
    for d in range(3, planes):
        w_forward(d, 0)
    for q in range(2, parts):
        pass_d(q)
    for d in range(3, planes):
        w_forward(d, 1)

    def product(slab):
        acc = None
        for zb in range(planes):
            got = lax.dot_general(
                cols[slab, zb], wh[zb], (((1,), (1,)), ((), ())), preferred_element_type=f32
            )
            acc = got if acc is None else acc + got
        return acc

    part_x = [
        [copy(part_out.at[n, h], part_in.at[n, h], "part_x", 2 * n + h, to_x) for h in range(2)]
        for n in range(2)
    ]
    cut = side // 2

    def partial(slab, n):
        got = product(slab)
        for h in range(2):
            part_out[n, h] = got[:, h * cut : (h + 1) * cut].astype(bf16)
            send(part_x[n][h])

    for q in range(1, parts):
        arrive(cols_core(3, "cols_d_core", q))
    partial(3, 1)
    for q in range(1, parts):
        arrive(cols_core(1, "cols_x_core", q))
    partial(1, 0)
    pass_y(1)
    part[0] = product(0)
    arrive(cols_core(2, "cols_y_core", 1))
    weight_of(turn[1])
    fresh(1, 0)
    serve_near(0)
    for q in range(2, parts):
        pass_y(q)
    for q in range(2, parts):
        arrive(cols_core(2, "cols_y_core", q))
    part[1] = product(2)
    part_y = [copy(half_out.at[h], half_in.at[h], "part_y", h, to_y) for h in range(2)]

    def fold(h):
        arrive(part_x[1][h])
        got = part[1, :, h * cut : (h + 1) * cut] + part_in[1, h].astype(f32)
        half_out[h] = got.astype(bf16)
        send(part_y[h])

    fold(0)
    for q in range(2, planes - 1):
        weight_of(turn[q])
        fresh(q, 0)
        fresh(q - 1, 1)
    serve_near(1)
    serve_far(0)
    fold(1)
    weight_of(turn[planes - 1])
    stat_out[2] = jnp.zeros((rows, LANES), f32)
    stat_out[3] = jnp.zeros((rows, LANES), f32)

    def back_tile(j, got):
        pre_grad = got * dact[j]
        normed = conv[j]
        scaled = pre_grad * gain[0:1, lanes(j)]
        crossed = pre_grad * normed
        dact[j] = scaled
        stat_out[2] = stat_out[2] + scaled
        stat_out[3] = stat_out[3] + scaled * normed
        small[j, span : span + 1, :] = jnp.sum(crossed, axis=0, keepdims=True)
        small[j, span + 1 : span + 2, :] = jnp.sum(pre_grad, axis=0, keepdims=True)

    tiles_cut = tiles_side // 2

    def back_mine(h):
        arrive(part_x[0][h])

        def one(jj):
            at_side = lanes(h * tiles_cut + jj)
            got = part[0, :, at_side] + part_in[0, h, :, lanes(jj)].astype(f32)
            back_tile(y * tiles_side + h * tiles_cut + jj, got)

        over(tiles_cut, one)

    def back_theirs(h):
        arrive(part_y[h])

        def one(jj):
            back_tile(yn * tiles_side + h * tiles_cut + jj, half_in[h, :, lanes(jj)].astype(f32))

        over(tiles_cut, one)

    back_mine(0)
    serve_near(2)
    back_theirs(0)
    back_mine(1)
    back_theirs(1)
    norm = copy(stat_out.at[2:4], stat_in.at[2:4], "norm", 0, to_core)
    send(norm)
    serve_far(1)
    arrive(norm)
    for r in range(0, rows, step):
        at_rows = slice(r, r + step)
        for n in range(2):
            both = stat_out[2 + n, at_rows, :] + stat_in[2 + n, at_rows, :]
            got = jnp.sum(both, axis=1, keepdims=True) / (2 * width)
            rows_of[2 + n, at_rows, :] = jnp.broadcast_to(got, (step, LANES))

    def grad_tile(j):
        grads[j, EDGE : EDGE + rows, :] = rows_of[1] * (
            dact[j] - rows_of[2] - conv[j] * rows_of[3]
        )
        gedge_out[0, j] = grads[j, rows : rows + EDGE, :]
        gedge_out[1, j] = grads[j, EDGE : 2 * EDGE, :]

    over(tiles, grad_tile)
    grad_prev = copy(gedge_out.at[0], gedge_in.at[0], "grad_halo", 0, to_next)
    grad_next = copy(gedge_out.at[1], gedge_in.at[1], "grad_halo", 1, to_prev)
    send(grad_prev, has_next)
    send(grad_next, has_prev)

    def tap_tile(j):
        for at in range(0, span, GROUP):
            ks = range(at, min(at + GROUP, span))
            acc = {}
            for r in range(0, rows, step):
                own = grads[j, r + EDGE : r + EDGE + step, :]
                for k in ks:
                    got = own * mixed[j, r + k + lead : r + k + lead + step, :]
                    folded = jnp.sum(got.reshape(step // 8, 8, LANES), axis=0)
                    acc[k] = acc[k] + folded if k in acc else folded
            for k in ks:
                small[j, k : k + 1, :] = jnp.sum(acc[k], axis=0, keepdims=True)

    place = 2 * y + x
    near = [(to_d, 2 * yn + xn), (to_x, 2 * y + xn), (to_y, 2 * yn + x)]
    own_tiles = pl.ds(place * quarter, quarter)
    gather = [
        copy(small.at[pl.ds(p * quarter, quarter)], plane_in.at[n], "plane_in", n, dev)
        for n, (dev, p) in enumerate(near)
    ]
    for n, (dev, p) in enumerate(near):
        over(quarter, lambda jj: tap_tile(p * quarter + jj))
        send(gather[n])
    over(quarter, lambda jj: tap_tile(place * quarter + jj))
    finish(0)
    send(back)

    def mixed_tile(j):
        for r in range(0, rows, step):
            at_row = r + EDGE + half
            acc = tap_t[j, 0:1, :] * grads[j, at_row : at_row + step, :]
            for k in range(1, span):
                at_row = r + EDGE + half - k
                acc = acc + tap_t[j, k : k + 1, :] * grads[j, at_row : at_row + step, :]
            tile[r : r + step, :] = acc
        got = tile[...]
        value_v[:, lanes(j)] = (got * factor_v[j]).astype(bf16)
        gate_v[:, lanes(j)] = (got * factor_g[j]).astype(bf16)

    def mixed_tiles(lo, hi):
        lax.fori_loop(lo, hi, lambda j, c: (mixed_tile(j), c)[1], 0)

    def across_out():
        for d in range(1, planes):
            arrive(copy(across.at[z], across.at[z], "across", d, to_core))
        total = across[0].astype(f32)
        for d in range(1, planes):
            total = total + across[d].astype(f32)
        owned[...] = total
        small_all[own_tiles] = total
        for made in spread_out:
            send(made)

    spread_out = [
        copy(owned, small_all.at[own_tiles], "plane_out", n, dev) for n, (dev, p) in enumerate(near)
    ]
    for made in gather:
        arrive(made)
    joined = small[own_tiles] + plane_in[0] + plane_in[1] + plane_in[2]
    across[z] = joined.astype(bf16)
    for d in range(1, planes):
        made = copy(across.at[z], across.at[z], "across", d, at(lax.rem(z + d, planes), y, x))
        send(made)
    for n in range(3, 2 * (planes - 1)):
        serve_near(n)
        serve_far(n - 1)
    serve_far(2 * planes - 3)
    for m in range(2, planes - 1):
        fresh(m, 1)
    fill(grad_prev, has_prev, gedge_in.at[0], grads, 0)
    fill(grad_next, has_next, gedge_in.at[1], grads, EDGE + rows)
    mixed_tiles(0, 3 * quarter)
    across_out()
    mixed_tiles(3 * quarter, tiles)
    stores = [
        pltpu.make_async_copy(value_v, value_grad, local_sem.at[0]),
        pltpu.make_async_copy(gate_v, gate_grad, local_sem.at[1]),
        pltpu.make_async_copy(weight_v, weight_mine, local_sem.at[2]),
        pltpu.make_async_copy(small_all, small_grad, local_sem.at[3]),
        pltpu.make_async_copy(back_in, weight_back, local_sem.at[4]),
    ]
    stores[0].start()
    stores[1].start()

    finish(1)
    stores[2].start()
    for made in spread_out:
        arrive(made)
    stores[3].start()
    arrive(back)
    stores[4].start()
    for made, when in pending:
        if when is None:
            made.wait_send()
        else:
            pl.when(when)(made.wait_send)
    for made in stores:
        made.wait()


def write_out(
    span,
    value_in,
    gate_in,
    small_in,
    mine_in,
    back_in,
    value_out,
    gate_out,
    tap_out,
    gain_out,
    bias_out,
    weight_out,
    value_v,
    gate_v,
    small_v,
    mine_v,
    back_v,
    tap_v,
    gain_v,
    bias_v,
    wide_v,
    in_sem,
    out_sem,
):
    side = mine_v.shape[0]
    tiles = small_v.shape[0]
    y = lax.rem(lax.div(lax.axis_index("sp"), 2), 2)

    def rows_at(h):
        return pl.ds(pl.multiple_of(h * side, side), side)

    pairs = (
        (back_in, back_v),
        (small_in, small_v),
        (value_in, value_v),
        (gate_in, gate_v),
        (mine_in, mine_v),
    )
    loads = [pltpu.make_async_copy(a, b, in_sem.at[n]) for n, (a, b) in enumerate(pairs)]
    pairs = (
        (wide_v, weight_out.at[rows_at(1 - y)]),
        (tap_v, tap_out),
        (gain_v, gain_out),
        (bias_v, bias_out),
        (value_v, value_out),
        (gate_v, gate_out),
        (mine_v, weight_out.at[rows_at(y)]),
    )
    stores = [pltpu.make_async_copy(a, b, out_sem.at[n]) for n, (a, b) in enumerate(pairs)]
    for made in loads:
        made.start()
    loads[0].wait()
    wide_v[...] = back_v[...].astype(jnp.float32)
    stores[0].start()
    loads[1].wait()
    for j in range(tiles):
        at_lanes = slice(j * LANES, (j + 1) * LANES)
        tap_v[:, at_lanes] = small_v[j, 0:span, :]
        gain_v[:, at_lanes] = small_v[j, span : span + 1, :]
        bias_v[:, at_lanes] = small_v[j, span + 1 : span + 2, :]
    for n in (1, 2, 3):
        stores[n].start()
    for n in (2, 3, 4):
        loads[n].wait()
        stores[n + 2].start()
    for made in stores:
        made.wait()


def fused_on_device(value_in, gate_in, taps, norm_gain, norm_bias, proj_weight, out_grad):
    f32, bf16 = jnp.float32, jnp.bfloat16
    rows, width = value_in.shape
    span = taps.shape[0]
    block = proj_weight.shape[1]
    planes = lax.axis_size("sp") // 4
    blocks = 2 * planes
    side = width // 2
    tiles = width // LANES
    step = max(n for n in (8, 16, 24, 32, 40) if rows % n == 0)
    kept = -(-(span + 2) // 8) * 8
    first, total = slot_table(planes, blocks)
    vmem, dma = pltpu.VMEM, pltpu.SemaphoreType.DMA
    scratch = [
        vmem((rows, width), bf16),
        vmem((rows, width), bf16),
        vmem((span, width), f32),
        vmem((1, width), f32),
        vmem((1, width), f32),
        vmem((4, planes, rows, 2 * block), bf16),
        vmem((planes, side, 2 * block), bf16),
        vmem((tiles, kept, LANES), f32),
        vmem((tiles, rows + 2 * EDGE, LANES), f32),
        vmem((4, EDGE, width), bf16),
        vmem((tiles, rows, LANES), f32),
        vmem((tiles, rows, LANES), f32),
        vmem((4, rows, LANES), f32),
        vmem((4, rows, LANES), f32),
        vmem((4, rows, LANES), f32),
        vmem((5, rows, side), bf16),
        vmem((tiles, rows, LANES), f32),
        vmem((tiles, rows, LANES), f32),
        vmem((2, rows, side), f32),
        vmem((2, 2, rows, side // 2), bf16),
        vmem((2, 2, rows, side // 2), bf16),
        vmem((2, rows, side // 2), bf16),
        vmem((2, rows, side // 2), bf16),
        vmem((blocks, side, block), f32),
        vmem((blocks, side, block), bf16),
        vmem((blocks, side, block), bf16),
        vmem((blocks, side, block), bf16),
        vmem((blocks, side, block), bf16),
        vmem((side, block), bf16),
        vmem((side, block), bf16),
        vmem((side, block), f32),
        vmem((4, side, rows), bf16),
        vmem((tiles, rows + 2 * EDGE, LANES), f32),
        vmem((2, tiles, EDGE, LANES), f32),
        vmem((2, tiles, EDGE, LANES), f32),
        vmem((tiles, kept, LANES), f32),
        vmem((3, tiles // 4, kept, LANES), f32),
        vmem((planes, tiles // 4, kept, LANES), bf16),
        vmem((tiles // 4, kept, LANES), f32),
        vmem((tiles, kept, LANES), f32),
        vmem((rows, LANES), f32),
        dma((total,)),
        dma((total,)),
        dma((6 + blocks,)),
    ]
    hbm = pl.BlockSpec(memory_space=pl.ANY)
    values = jax.ShapeDtypeStruct((rows, width), bf16)
    given = pl.pallas_call(
        functools.partial(kernel, (rows, width, span, planes, block, step), first),
        out_shape=(
            values,
            values,
            jax.ShapeDtypeStruct((tiles, kept, LANES), f32),
            jax.ShapeDtypeStruct((side, block), f32),
            jax.ShapeDtypeStruct((side, block), bf16),
        ),
        in_specs=[hbm] * 7,
        out_specs=[hbm] * 5,
        scratch_shapes=scratch,
        compiler_params=pltpu.CompilerParams(
            collective_id=0, has_side_effects=True, vmem_limit_bytes=62 * 2**20
        ),
    )(
        value_in,
        gate_in,
        taps,
        norm_gain.reshape(1, width),
        norm_bias.reshape(1, width),
        proj_weight,
        out_grad,
    )
    value_grad, gate_grad, tap_grad, gain_grad, bias_grad, weight_grad = pl.pallas_call(
        functools.partial(write_out, span),
        out_shape=(
            values,
            values,
            jax.ShapeDtypeStruct((span, width), f32),
            jax.ShapeDtypeStruct((1, width), f32),
            jax.ShapeDtypeStruct((1, width), f32),
            jax.ShapeDtypeStruct((width, block), f32),
        ),
        in_specs=[hbm] * 5,
        out_specs=[hbm] * 6,
        scratch_shapes=[
            vmem((rows, width), bf16),
            vmem((rows, width), bf16),
            vmem((tiles, kept, LANES), f32),
            vmem((side, block), f32),
            vmem((side, block), bf16),
            vmem((span, width), f32),
            vmem((1, width), f32),
            vmem((1, width), f32),
            vmem((side, block), f32),
            dma((5,)),
            dma((7,)),
        ],
        compiler_params=pltpu.CompilerParams(vmem_limit_bytes=62 * 2**20),
    )(*given)
    return (
        value_grad,
        gate_grad,
        tap_grad,
        gain_grad.reshape(width),
        bias_grad.reshape(width),
        weight_grad,
    )


def solution(mesh):
    fused = mesh.shape["tp"] == 2 and mesh.shape["sp"] % 4 == 0
    return jax.shard_map(
        fused_on_device if fused else on_device,
        mesh=mesh,
        in_specs=(
            P("sp", "tp"),
            P("sp", "tp"),
            P(None, "tp"),
            P("tp"),
            P("tp"),
            P("tp", "sp"),
            P("sp", None),
        ),
        out_specs=(P("sp", "tp"), P("sp", "tp"), P(None, "tp"), P("tp"), P("tp"), P("tp", "sp")),
        check_vma=False,
    )
```

```python
import functools
import jax
import jax.numpy as jnp
from jax import lax
from jax.experimental import pallas as pl
from jax.experimental.pallas import tpu as pltpu
from jax.sharding import PartitionSpec as P


def padded_rows(cells, width):
    count = lax.axis_size("sp")
    ends = count - 1
    rows = cells.shape[0]
    before = lax.ppermute(cells[rows - width :], "sp", [(i, i + 1) for i in range(ends)])
    after = lax.ppermute(cells[:width], "sp", [(i + 1, i) for i in range(ends)])
    return jnp.concatenate([before, cells, after], axis=0)


def on_device(*arrays):
    return compute(*arrays)


def compute(value_in, gate_in, taps, norm_gain, norm_bias, proj_weight, out_grad):
    f32, bf16 = jnp.float32, jnp.bfloat16
    rows, local_width = value_in.shape
    span = taps.shape[0]
    half = span // 2
    tp = lax.axis_size("tp")
    count = lax.axis_size("sp")
    inner = 1 << ((count.bit_length() - 1) // 2)
    outer = count // inner
    width_all = local_width * tp
    block = proj_weight.shape[1]
    me = lax.axis_index("sp")
    plane, place = me // inner, me % inner
    core = lax.axis_index("tp")

    def swap(array, d):
        return lax.ppermute(
            array, "sp", [(i, i - i % inner + ((i % inner) ^ d)) for i in range(count)]
        )

    def shift(array, e):
        return lax.ppermute(array, "sp", [(i, (i + e * inner) % count) for i in range(count)])

    def across(array, t):
        return lax.ppermute(array, "tp", [(c, c ^ t) for c in range(tp)])

    def tp_sum(array):
        return array + sum(across(array, t) for t in range(1, tp))

    gate_sig = jax.nn.sigmoid(gate_in.astype(f32))
    value_f = value_in.astype(f32)
    mixed = (value_f * gate_sig).astype(bf16)
    padded = padded_rows(mixed, half).astype(f32)

    def columns_of(where, first, blocks):
        return jnp.concatenate(
            [
                lax.dynamic_slice_in_dim(
                    out_grad,
                    (((plane + first + e) % outer) * inner + where) * block,
                    block,
                    axis=1,
                )
                for e in range(blocks)
            ],
            axis=1,
        )

    share = outer // tp
    own_columns = columns_of(place, 0, outer)
    arrived = [swap(columns_of(place ^ d, core * share, share), d) for d in range(1, inner)]
    weights = [proj_weight] + [shift(proj_weight, -e) for e in range(1, outer)]
    weight_cols = jnp.concatenate(weights, axis=1)
    cotangents = [own_columns]
    for got in arrived:
        parts = jnp.stack([got] + [across(got, t) for t in range(1, tp)])
        cotangents.append(
            jnp.concatenate(
                [
                    lax.dynamic_index_in_dim(parts, core ^ j, axis=0, keepdims=False)
                    for j in range(tp)
                ],
                axis=1,
            )
        )

    conv = jnp.zeros((rows, local_width), f32)
    for k in range(span):
        conv = conv + taps[k] * padded[k : k + rows]
    mean = tp_sum(jnp.sum(conv, axis=1)) / width_all
    centred = conv - mean[:, None]
    spread = tp_sum(jnp.sum(centred * centred, axis=1)) / width_all
    inv = lax.rsqrt(spread + 1e-06)
    normed = centred * inv[:, None]
    pre = normed * norm_gain + norm_bias
    sig_pre = jax.nn.sigmoid(pre)
    act = (pre * sig_pre).astype(bf16)
    acts = [act] + [swap(act, d) for d in range(1, inner)]

    partial = [
        lax.dot_general(c, weight_cols, (((1,), (1,)), ((), ())), preferred_element_type=f32)
        for c in cotangents
    ]
    act_grad = partial[0]
    sending = lax.optimization_barrier(([p.astype(bf16) for p in partial[1:]], acts))[0]
    for d in range(1, inner):
        got = swap(sending[d - 1], d)
        act_grad = act_grad + got.astype(f32)

    pre_grad = act_grad * sig_pre * (1.0 + pre * (1.0 - sig_pre))
    normed_grad = pre_grad * norm_gain
    sums = tp_sum(
        jnp.stack([jnp.sum(normed_grad, axis=1), jnp.sum(normed_grad * normed, axis=1)])
    )
    first, second = sums[0], sums[1]
    conv_grad = inv[:, None] * (
        normed_grad - first[:, None] / width_all - normed * second[:, None] / width_all
    )
    extended = lax.optimization_barrier(padded_rows(conv_grad, half))
    tap_local = jnp.stack([jnp.sum(conv_grad * padded[k : k + rows], axis=0) for k in range(span)])
    gain_local = jnp.sum(pre_grad * normed, axis=0)
    bias_local = jnp.sum(pre_grad, axis=0)
    small = jnp.concatenate([tap_local, gain_local[None], bias_local[None]], axis=0)
    small = small + sum(swap(small, d) for d in range(1, inner))
    small = small + sum(shift(small, e) for e in range(1, outer))
    tap_grad, gain_grad, bias_grad = small[:span], small[span], small[span + 1]

    mixed_grad = jnp.zeros((rows, local_width), f32)
    for k in range(span):
        mixed_grad = mixed_grad + taps[k] * extended[2 * half - k : 2 * half - k + rows]
    value_grad = (mixed_grad * gate_sig).astype(bf16)
    gate_grad = (mixed_grad * value_f * gate_sig * (1.0 - gate_sig)).astype(bf16)

    weight_part = lax.dot_general(
        jnp.concatenate(acts, axis=0),
        jnp.concatenate(cotangents, axis=0),
        (((0,), (0,)), ((), ())),
        preferred_element_type=f32,
    )
    weight_grad = weight_part[:, :block]
    for e in range(1, outer):
        sent = weight_part[:, e * block : (e + 1) * block].astype(bf16)
        got = shift(sent, e)
        weight_grad = weight_grad + got.astype(f32)
    return (value_grad, gate_grad, tap_grad, gain_grad, bias_grad, weight_grad)


LANES = 128
EDGE = 16
GROUP = 16
MESH = pl.DeviceIdType.MESH


def slot_table(planes, blocks):
    parts = blocks // 2
    sizes = {
        "halo": 4,
        "cols_x": parts,
        "cols_x_core": parts,
        "cols_d": parts,
        "cols_d_core": parts,
        "cols_y": parts,
        "cols_y_core": parts,
        "w_y": 1,
        "w_up": 2 * (planes - 1),
        "w_down": 2 * (planes - 1),
        "stats": 1,
        "act_x": 1,
        "act_y": 1,
        "act_d": 1,
        "part_x": 4,
        "part_y": 2,
        "up": blocks,
        "down": blocks,
        "w_back": 1,
        "norm": 1,
        "grad_halo": 2,
        "plane_in": 3,
        "across": planes,
        "plane_out": 3,
    }
    first, total = {}, 0
    for name, size in sizes.items():
        first[name] = total
        total += size
    return first, total


def kernel(
    shape,
    first,
    value,
    gate,
    taps_hbm,
    gain_hbm,
    bias_hbm,
    weight,
    cotangent,
    value_grad,
    gate_grad,
    small_grad,
    weight_mine,
    weight_back,
    value_v,
    gate_v,
    taps,
    gain,
    bias,
    cols,
    wh,
    tap_t,
    mixed,
    edge_in,
    conv,
    dact,
    stat_out,
    stat_in,
    rows_of,
    acts,
    factor_v,
    factor_g,
    part,
    part_out,
    part_in,
    half_out,
    half_in,
    wg,
    up_out,
    down_out,
    up_in,
    down_in,
    back_out,
    back_in,
    weight_v,
    turned,
    grads,
    gedge_out,
    gedge_in,
    small,
    plane_in,
    across,
    owned,
    small_all,
    tile,
    narrow,
    send_sem,
    recv_sem,
    local_sem,
):
    rows, width, span, planes, block, step = shape
    f32, bf16 = jnp.float32, jnp.bfloat16
    blocks = 2 * planes
    parts = blocks // 2
    side = width // 2
    tiles = width // LANES
    tiles_side = tiles // 2
    quarter = tiles // 4
    count = 4 * planes
    half = span // 2
    lead = EDGE - half

    me, core = lax.axis_index("sp"), lax.axis_index("tp")
    z, y, x = lax.div(me, 4), lax.rem(lax.div(me, 2), 2), lax.rem(me, 2)
    yn, xn = 1 - y, 1 - x

    def at(zz, yy, xx):
        return (zz * 4 + yy * 2 + xx, core)

    to_x, to_y, to_d = at(z, y, xn), at(z, yn, x), at(z, yn, xn)
    to_core = (me, 1 - core)
    to_up, to_down = (me + 4, core), (me - 4, core)
    to_next, to_prev = (me + 1, core), (me - 1, core)
    has_up, has_down = z < planes - 1, z > 0
    has_next, has_prev = me < count - 1, me > 0

    pending = []

    def copy(src, dst, name, index, device):
        at_slot = first[name] + index
        return pltpu.make_async_remote_copy(
            src_ref=src,
            dst_ref=dst,
            send_sem=send_sem.at[at_slot],
            recv_sem=recv_sem.at[at_slot],
            device_id=device,
            device_id_type=MESH,
        )

    def send(made, when=None):
        pending.append((made, when))
        if when is None:
            made.start()
        else:
            pl.when(when)(made.start)

    def arrive(made, when=None):
        if when is None:
            made.wait_recv()
        else:
            pl.when(when)(made.wait_recv)

    def lanes(j):
        return pl.ds(pl.multiple_of(j * LANES, LANES), LANES)

    def over(n, body):
        def step_of(j, carry):
            body(j)
            return carry

        lax.fori_loop(0, n, step_of, 0)

    my_rows = pl.ds(pl.multiple_of(y * side, side), side)
    their_rows = pl.ds(pl.multiple_of(yn * side, side), side)

    def column(b):
        return pl.ds(pl.multiple_of(b * block, block), block)

    low = 2 * z < planes
    turn = []
    for q in range(planes - 1):
        down_to = planes - 1 - q
        fall = down_to - jnp.where(down_to <= z, 1, 0)
        rise = q + jnp.where(q >= z, 1, 0)
        turn.append(jnp.where(low, fall, rise))
    turn.append(z)
    mine = [2 * zb + core for zb in turn]

    def cols_at(slab, i):
        return cols.at[slab, lax.div(i, 2), :, column(lax.rem(i, 2))]

    def wh_at(zz, yy):
        return wh.at[zz, :, column(yy)]

    load_v = pltpu.make_async_copy(value, value_v, local_sem.at[0])
    load_g = pltpu.make_async_copy(gate, gate_v, local_sem.at[1])
    load_w = pltpu.make_async_copy(weight.at[my_rows], wh_at(z, y), local_sem.at[2])
    load_c = [
        pltpu.make_async_copy(
            cotangent.at[:, column(2 * i + x)],
            cols.at[0, i // 2, :, (i % 2) * block : (i % 2 + 1) * block],
            local_sem.at[3 + i],
        )
        for i in range(blocks)
    ]
    load_s = [
        pltpu.make_async_copy(src, dst, local_sem.at[3 + blocks + n])
        for n, (src, dst) in enumerate(((taps_hbm, taps), (gain_hbm, gain), (bias_hbm, bias)))
    ]

    barrier = pltpu.get_barrier_semaphore()
    peers = [to_x, to_y, to_d, to_core]
    peers += [at(lax.rem(z + d, planes), y, x) for d in range(1, planes)]
    peers += [(lax.rem(me + 1, count), core), (lax.rem(me + count - 1, count), core)]
    for peer in peers:
        pl.semaphore_signal(barrier, inc=1, device_id=peer, device_id_type=MESH)
    load_v.start()
    load_g.start()
    for made in load_s:
        made.start()

    def w_copies(d, p):
        yb = y if p == 0 else yn
        index = 2 * (d - 1) + p
        below = wh_at(lax.rem(z - d + planes, planes), yb)
        above = wh_at(lax.rem(z + d, planes), yb)
        return (
            copy(below, below, "w_up", index, to_up),
            copy(above, above, "w_down", index, to_down),
        )

    def w_first(p, src, yb):
        dst = wh_at(z, yb)
        send(copy(src, dst, "w_up", p, to_up), has_up)
        send(copy(src, dst, "w_down", p, to_down), has_down)

    def w_forward(d, p):
        up, down = w_copies(d, p)
        yb = y if p == 0 else yn
        below = wh_at(lax.rem(z - d + planes, planes), yb)
        above = wh_at(lax.rem(z + d, planes), yb)
        arrive(up, z >= d)
        if d < planes - 1:
            send(copy(below, below, "w_up", 2 * d + p, to_up), jnp.logical_and(z >= d, has_up))
        arrive(down, z + d < planes)
        if d < planes - 1:
            send(
                copy(above, above, "w_down", 2 * d + p, to_down),
                jnp.logical_and(z + d < planes, has_down),
            )

    w_y = copy(weight.at[their_rows], wh_at(z, y), "w_y", 0, to_y)

    def cols_x(q):
        return copy(
            cotangent.at[:, column(2 * mine[q] + xn)], cols_at(1, mine[q]), "cols_x", q, to_x
        )

    def cols_d(q):
        return copy(cols_at(1, mine[q]), cols_at(3, mine[q]), "cols_d", q, to_y)

    def cols_y(q):
        return copy(
            cotangent.at[:, column(2 * mine[q] + x)], cols_at(2, mine[q]), "cols_y", q, to_y
        )

    def cols_core(slab, name, q):
        ref = cols_at(slab, mine[q])
        return copy(ref, ref, name, q, to_core)

    def pass_x(q):
        arrive(cols_x(q))
        send(cols_d(q))
        send(cols_core(1, "cols_x_core", q))

    def pass_d(q):
        arrive(cols_d(q))
        send(cols_core(3, "cols_d_core", q))

    def pass_y(q):
        arrive(cols_y(q))
        send(cols_core(2, "cols_y_core", q))

    pl.semaphore_wait(barrier, len(peers))
    halo = []
    for n, (src, near_rows) in enumerate(
        ((value, rows - EDGE), (gate, rows - EDGE), (value, 0), (gate, 0))
    ):
        made = copy(
            src.at[near_rows : near_rows + EDGE],
            edge_in.at[n],
            "halo",
            n,
            to_next if n < 2 else to_prev,
        )
        send(made, has_next if n < 2 else has_prev)
        halo.append(made)
    w_first(0, weight.at[my_rows], y)
    send(w_y)
    send(cols_y(0))
    for q in range(parts):
        send(cols_x(q))
    load_w.start()
    for made in load_c:
        made.start()
    for made in load_s:
        made.wait()
    load_v.wait()
    load_g.wait()

    def gate_tile(j):
        tap_t[j, 0:span, :] = taps[:, lanes(j)]
        small[j] = jnp.zeros(small.shape[1:], f32)
        sig = jax.nn.sigmoid(gate_v[:, lanes(j)].astype(f32))
        got = (value_v[:, lanes(j)].astype(f32) * sig).astype(bf16).astype(f32)
        mixed[j, EDGE : EDGE + rows, :] = got

    over(tiles, gate_tile)

    def fill(made, when, src, dst, at_row):
        @pl.when(when)
        def _():
            made.wait_recv()
            for j in range(tiles):
                dst[j, at_row : at_row + EDGE, :] = src[j].astype(f32)

        @pl.when(jnp.logical_not(when))
        def _():
            for j in range(tiles):
                dst[j, at_row : at_row + EDGE, :] = jnp.zeros((EDGE, LANES), f32)

    def fill_mixed(first_of, when, at_row):
        @pl.when(when)
        def _():
            halo[first_of].wait_recv()
            halo[first_of + 1].wait_recv()
            for j in range(tiles):
                at_lanes = slice(j * LANES, (j + 1) * LANES)
                sig = jax.nn.sigmoid(edge_in[first_of + 1, :, at_lanes].astype(f32))
                got = edge_in[first_of, :, at_lanes].astype(f32) * sig
                mixed[j, at_row : at_row + EDGE, :] = got.astype(bf16).astype(f32)

        @pl.when(jnp.logical_not(when))
        def _():
            for j in range(tiles):
                mixed[j, at_row : at_row + EDGE, :] = jnp.zeros((EDGE, LANES), f32)

    fill_mixed(0, has_prev, 0)
    fill_mixed(2, has_next, EDGE + rows)

    def conv_tile(j):
        for r in range(0, rows, step):
            acc = tap_t[j, 0:1, :] * mixed[j, r + lead : r + lead + step, :]
            for k in range(1, span):
                at_row = r + k + lead
                acc = acc + tap_t[j, k : k + 1, :] * mixed[j, at_row : at_row + step, :]
            conv[j, r : r + step, :] = acc

    over(tiles, conv_tile)
    for r in range(0, rows, step):
        at_rows = slice(r, r + step)
        total = conv[0, at_rows, :]
        for j in range(1, tiles):
            total = total + conv[j, at_rows, :]
        middle = jnp.sum(total, axis=1, keepdims=True) / width
        off = conv[0, at_rows, :] - middle
        square = off * off
        for j in range(1, tiles):
            off = conv[j, at_rows, :] - middle
            square = square + off * off
        stat_out[0, at_rows, :] = total
        stat_out[1, at_rows, :] = square
    stats = copy(stat_out.at[0:2], stat_in.at[0:2], "stats", 0, to_core)
    send(stats)
    arrive(w_y)
    w_first(1, wh_at(z, yn), yn)
    w_forward(1, 0)
    arrive(stats)
    for r in range(0, rows, step):
        at_rows = slice(r, r + step)
        here = jnp.sum(stat_out[0, at_rows, :], axis=1, keepdims=True)
        there = jnp.sum(stat_in[0, at_rows, :], axis=1, keepdims=True)
        both = stat_out[1, at_rows, :] + stat_in[1, at_rows, :]
        apart = (here - there) / width
        spread = jnp.sum(both, axis=1, keepdims=True) / (2 * width) + apart * apart / 4
        inv = lax.rsqrt(spread + 1e-06)
        rows_of[0, at_rows, :] = jnp.broadcast_to((here + there) / (2 * width), (step, LANES))
        rows_of[1, at_rows, :] = jnp.broadcast_to(inv, (step, LANES))

    def act_side(h):
        def act_tile(jj):
            j = h * tiles_side + jj
            normed = (conv[j] - rows_of[0]) * rows_of[1]
            pre = normed * gain[0:1, lanes(j)] + bias[0:1, lanes(j)]
            sig = jax.nn.sigmoid(pre)
            acts[h, :, lanes(jj)] = (pre * sig).astype(bf16)
            conv[j] = normed
            dact[j] = sig * (1.0 + pre * (1.0 - sig))

        over(tiles_side, act_tile)

    act_y = copy(acts.at[yn], acts.at[3], "act_y", 0, to_y)
    act_x = copy(acts.at[y], acts.at[2], "act_x", 0, to_x)
    act_d = copy(acts.at[3], acts.at[4], "act_d", 0, to_x)
    act_side(yn)
    send(act_y)
    act_side(y)
    send(act_x)
    pass_x(0)
    pass_x(1)
    pass_y(0)
    for q in range(2, parts - 1):
        pass_x(q)
    w_forward(1, 1)
    pass_x(parts - 1)
    for q in range(1, parts):
        send(cols_y(q))

    def factor_tile(j):
        sig = jax.nn.sigmoid(gate_v[:, lanes(j)].astype(f32))
        factor_v[j] = sig
        factor_g[j] = value_v[:, lanes(j)].astype(f32) * sig * (1.0 - sig)

    over(tiles, factor_tile)
    turned[0] = acts[y].T
    arrive(act_y)
    send(act_d)
    if planes > 2:
        w_forward(2, 0)
    arrive(act_x)
    turned[1] = acts[2].T
    turned[2] = acts[3].T
    pass_d(0)
    if planes > 2:
        w_forward(2, 1)
    pass_d(1)
    load_w.wait()
    for made in load_c:
        made.wait()

    def weight_of(zb, lo=0, hi=4):
        acc = None
        for slab in range(lo, hi):
            got = jnp.dot(turned[slab], cols[slab, zb], preferred_element_type=f32)
            acc = got if acc is None else acc + got
        for n in range(2):
            got = acc[:, n * block : (n + 1) * block]
            wg[2 * zb + n] = got if lo == 0 else wg[2 * zb + n] + got

    def up_copy(t, p):
        i = 2 * t + (yn if p == 0 else y)
        return copy(up_out.at[i], up_in.at[i], "up", 2 * t + p, to_up)

    def down_copy(t, p):
        i = 2 * t + (yn if p == 0 else y)
        return copy(down_out.at[i], down_in.at[i], "down", 2 * t + p, to_down)

    def fresh(m, p):
        for t, made, out, when in (
            (planes - 1 - m, up_copy(planes - 1 - m, p), up_out, z == 0),
            (m, down_copy(m, p), down_out, z == planes - 1),
        ):
            i = 2 * t + (yn if p == 0 else y)

            @pl.when(when)
            def _():
                out[i] = wg[i].astype(bf16)

            send(made, when)

    def finish(p):
        i = 2 * z + (yn if p == 0 else y)
        for t in range(planes):

            @pl.when(z == t)
            def _():
                total = wg[i]
                if t > 0:
                    up_copy(t, p).wait_recv()
                    total = total + up_in[i].astype(f32)
                if t < planes - 1:
                    down_copy(t, p).wait_recv()
                    total = total + down_in[i].astype(f32)
                if p == 0:
                    back_out[...] = total.astype(bf16)
                else:
                    weight_v[...] = total

    back = copy(back_out, back_in, "w_back", 0, to_y)
    inner = jnp.logical_and(has_up, has_down)
    lower = jnp.logical_and(inner, 2 * z < planes)
    upper = jnp.logical_and(inner, 2 * z >= planes)

    def relay(n, going_up, side_of):
        m, p = n // 2, n % 2
        t = planes - 1 - m if going_up else m
        if not 0 <= m < planes - 1:
            return
        i = 2 * t + (yn if p == 0 else y)
        made = up_copy(t, p) if going_up else down_copy(t, p)
        out, got = (up_out, up_in) if going_up else (down_out, down_in)
        when = jnp.logical_and(side_of, z < t if going_up else z > t)

        @pl.when(when)
        def _():
            made.wait_recv()
            out[i] = (wg[i] + got[i].astype(f32)).astype(bf16)

        send(made, when)

    def serve_near(n):
        relay(n, True, lower)
        relay(n, False, upper)

    def serve_far(n):
        relay(n, False, lower)
        relay(n, True, upper)

    arrive(cols_core(1, "cols_x_core", 0))
    arrive(cols_core(3, "cols_d_core", 0))
    arrive(cols_core(2, "cols_y_core", 0))
    weight_of(turn[0], 0, 3)
    arrive(act_d)
    turned[3] = acts[4].T
    weight_of(turn[0], 3, 4)
    fresh(0, 0)
    fresh(0, 1)
    for d in range(3, planes):
        w_forward(d, 0)
    for q in range(2, parts):
        pass_d(q)
    for d in range(3, planes):
        w_forward(d, 1)

    def product(slab, over_zb=range(planes)):
        acc = None
        for zb in over_zb:
            got = lax.dot_general(
                cols[slab, zb], wh[zb], (((1,), (1,)), ((), ())), preferred_element_type=f32
            )
            acc = got if acc is None else acc + got
        return acc

    part_x = [
        [copy(part_out.at[n, h], part_in.at[n, h], "part_x", 2 * n + h, to_x) for h in range(2)]
        for n in range(2)
    ]
    cut = side // 2

    def partial(slab, n):
        got = product(slab)
        for h in range(2):
            part_out[n, h] = got[:, h * cut : (h + 1) * cut].astype(bf16)
            send(part_x[n][h])

    for q in range(1, parts):
        arrive(cols_core(3, "cols_d_core", q))
    partial(3, 1)
    for q in range(1, parts):
        arrive(cols_core(1, "cols_x_core", q))
    partial(1, 0)
    pass_y(1)
    part[0] = product(0)
    arrive(cols_core(2, "cols_y_core", 1))
    weight_of(turn[1])
    fresh(1, 0)
    serve_near(0)
    for q in range(2, parts):
        if q == parts - 1:
            part[1] = product(2, turn[0 : parts - 1])
        pass_y(q)
        arrive(cols_core(2, "cols_y_core", q))
    part[1] = part[1] + product(2, turn[parts - 1 :])
    part_y = [copy(half_out.at[h], half_in.at[h], "part_y", h, to_y) for h in range(2)]

    def fold(h):
        arrive(part_x[1][h])
        got = part[1, :, h * cut : (h + 1) * cut] + part_in[1, h].astype(f32)
        half_out[h] = got.astype(bf16)
        send(part_y[h])

    fold(0)
    for q in range(2, planes - 1):
        weight_of(turn[q])
        fresh(q, 0)
        fresh(q - 1, 1)
    serve_near(1)
    serve_far(0)
    fold(1)
    weight_of(turn[planes - 1])
    stat_out[2] = jnp.zeros((rows, LANES), f32)
    stat_out[3] = jnp.zeros((rows, LANES), f32)

    def back_tile(j, got):
        pre_grad = got * dact[j]
        normed = conv[j]
        scaled = pre_grad * gain[0:1, lanes(j)]
        crossed = pre_grad * normed
        dact[j] = scaled
        stat_out[2] = stat_out[2] + scaled
        stat_out[3] = stat_out[3] + scaled * normed
        small[j, span : span + 1, :] = jnp.sum(crossed, axis=0, keepdims=True)
        small[j, span + 1 : span + 2, :] = jnp.sum(pre_grad, axis=0, keepdims=True)

    tiles_cut = tiles_side // 2

    def back_mine(h):
        arrive(part_x[0][h])

        def one(jj):
            at_side = lanes(h * tiles_cut + jj)
            got = part[0, :, at_side] + part_in[0, h, :, lanes(jj)].astype(f32)
            back_tile(y * tiles_side + h * tiles_cut + jj, got)

        over(tiles_cut, one)

    def back_theirs(h):
        arrive(part_y[h])

        def one(jj):
            back_tile(yn * tiles_side + h * tiles_cut + jj, half_in[h, :, lanes(jj)].astype(f32))

        over(tiles_cut, one)

    back_mine(0)
    serve_near(2)
    back_theirs(0)
    back_mine(1)
    back_theirs(1)
    norm = copy(stat_out.at[2:4], stat_in.at[2:4], "norm", 0, to_core)
    send(norm)
    serve_far(1)
    arrive(norm)
    for r in range(0, rows, step):
        at_rows = slice(r, r + step)
        for n in range(2):
            both = stat_out[2 + n, at_rows, :] + stat_in[2 + n, at_rows, :]
            got = jnp.sum(both, axis=1, keepdims=True) / (2 * width)
            rows_of[2 + n, at_rows, :] = jnp.broadcast_to(got, (step, LANES))

    def grad_tile(j):
        grads[j, EDGE : EDGE + rows, :] = rows_of[1] * (
            dact[j] - rows_of[2] - conv[j] * rows_of[3]
        )
        gedge_out[0, j] = grads[j, rows : rows + EDGE, :]
        gedge_out[1, j] = grads[j, EDGE : 2 * EDGE, :]

    over(tiles, grad_tile)
    grad_prev = copy(gedge_out.at[0], gedge_in.at[0], "grad_halo", 0, to_next)
    grad_next = copy(gedge_out.at[1], gedge_in.at[1], "grad_halo", 1, to_prev)
    send(grad_prev, has_next)
    send(grad_next, has_prev)

    def tap_tile(j):
        for at in range(0, span, GROUP):
            ks = range(at, min(at + GROUP, span))
            acc = {}
            for r in range(0, rows, step):
                own = grads[j, r + EDGE : r + EDGE + step, :]
                for k in ks:
                    got = own * mixed[j, r + k + lead : r + k + lead + step, :]
                    folded = jnp.sum(got.reshape(step // 8, 8, LANES), axis=0)
                    acc[k] = acc[k] + folded if k in acc else folded
            for k in ks:
                small[j, k : k + 1, :] = jnp.sum(acc[k], axis=0, keepdims=True)

    place = 2 * y + x
    near = [(to_d, 2 * yn + xn), (to_x, 2 * y + xn), (to_y, 2 * yn + x)]
    own_tiles = pl.ds(place * quarter, quarter)
    gather = [
        copy(narrow.at[pl.ds(p * quarter, quarter)], plane_in.at[n], "plane_in", n, dev)
        for n, (dev, p) in enumerate(near)
    ]
    for n, (dev, p) in enumerate(near):
        over(quarter, lambda jj: tap_tile(p * quarter + jj))
        theirs = pl.ds(p * quarter, quarter)
        narrow[theirs] = small[theirs].astype(bf16)
        send(gather[n])
    over(quarter, lambda jj: tap_tile(place * quarter + jj))
    finish(0)
    send(back)

    def mixed_tile(j):
        for r in range(0, rows, step):
            at_row = r + EDGE + half
            acc = tap_t[j, 0:1, :] * grads[j, at_row : at_row + step, :]
            for k in range(1, span):
                at_row = r + EDGE + half - k
                acc = acc + tap_t[j, k : k + 1, :] * grads[j, at_row : at_row + step, :]
            tile[r : r + step, :] = acc
        got = tile[...]
        value_v[:, lanes(j)] = (got * factor_v[j]).astype(bf16)
        gate_v[:, lanes(j)] = (got * factor_g[j]).astype(bf16)

    def mixed_tiles(lo, hi):
        lax.fori_loop(lo, hi, lambda j, c: (mixed_tile(j), c)[1], 0)

    def across_out():
        for d in range(1, planes):
            arrive(copy(across.at[z], across.at[z], "across", d, to_core))
        total = across[0].astype(f32)
        for d in range(1, planes):
            total = total + across[d].astype(f32)
        owned[...] = total
        small_all[own_tiles] = total
        for made in spread_out:
            send(made)

    spread_out = [
        copy(owned, small_all.at[own_tiles], "plane_out", n, dev) for n, (dev, p) in enumerate(near)
    ]
    for made in gather:
        arrive(made)
    joined = small[own_tiles]
    for n in range(3):
        joined = joined + plane_in[n].astype(f32)
    across[z] = joined.astype(bf16)
    for d in range(1, planes):
        made = copy(across.at[z], across.at[z], "across", d, at(lax.rem(z + d, planes), y, x))
        send(made)
    for n in range(3, 2 * (planes - 1)):
        serve_near(n)
        serve_far(n - 1)
    serve_far(2 * planes - 3)
    for m in range(2, planes - 1):
        fresh(m, 1)
    fill(grad_prev, has_prev, gedge_in.at[0], grads, 0)
    fill(grad_next, has_next, gedge_in.at[1], grads, EDGE + rows)
    mixed_tiles(0, 3 * quarter)
    across_out()
    mixed_tiles(3 * quarter, tiles)
    stores = [
        pltpu.make_async_copy(value_v, value_grad, local_sem.at[0]),
        pltpu.make_async_copy(gate_v, gate_grad, local_sem.at[1]),
        pltpu.make_async_copy(weight_v, weight_mine, local_sem.at[2]),
        pltpu.make_async_copy(small_all, small_grad, local_sem.at[3]),
        pltpu.make_async_copy(back_in, weight_back, local_sem.at[4]),
    ]
    stores[0].start()
    stores[1].start()

    finish(1)
    stores[2].start()
    for made in spread_out:
        arrive(made)
    stores[3].start()
    arrive(back)
    stores[4].start()
    for made, when in pending:
        if when is None:
            made.wait_send()
        else:
            pl.when(when)(made.wait_send)
    for made in stores:
        made.wait()


def write_out(
    span,
    value_in,
    gate_in,
    small_in,
    mine_in,
    back_in,
    value_out,
    gate_out,
    tap_out,
    gain_out,
    bias_out,
    weight_out,
    value_v,
    gate_v,
    small_v,
    mine_v,
    back_v,
    tap_v,
    gain_v,
    bias_v,
    wide_v,
    in_sem,
    out_sem,
):
    side = mine_v.shape[0]
    tiles = small_v.shape[0]
    y = lax.rem(lax.div(lax.axis_index("sp"), 2), 2)

    def rows_at(h):
        return pl.ds(pl.multiple_of(h * side, side), side)

    pairs = (
        (back_in, back_v),
        (small_in, small_v),
        (value_in, value_v),
        (gate_in, gate_v),
        (mine_in, mine_v),
    )
    loads = [pltpu.make_async_copy(a, b, in_sem.at[n]) for n, (a, b) in enumerate(pairs)]
    pairs = (
        (wide_v, weight_out.at[rows_at(1 - y)]),
        (tap_v, tap_out),
        (gain_v, gain_out),
        (bias_v, bias_out),
        (value_v, value_out),
        (gate_v, gate_out),
        (mine_v, weight_out.at[rows_at(y)]),
    )
    stores = [pltpu.make_async_copy(a, b, out_sem.at[n]) for n, (a, b) in enumerate(pairs)]
    for made in loads:
        made.start()
    loads[0].wait()
    wide_v[...] = back_v[...].astype(jnp.float32)
    stores[0].start()
    loads[1].wait()
    for j in range(tiles):
        at_lanes = slice(j * LANES, (j + 1) * LANES)
        tap_v[:, at_lanes] = small_v[j, 0:span, :]
        gain_v[:, at_lanes] = small_v[j, span : span + 1, :]
        bias_v[:, at_lanes] = small_v[j, span + 1 : span + 2, :]
    for n in (1, 2, 3):
        stores[n].start()
    for n in (2, 3, 4):
        loads[n].wait()
        stores[n + 2].start()
    for made in stores:
        made.wait()


def fused_on_device(value_in, gate_in, taps, norm_gain, norm_bias, proj_weight, out_grad):
    f32, bf16 = jnp.float32, jnp.bfloat16
    rows, width = value_in.shape
    span = taps.shape[0]
    block = proj_weight.shape[1]
    planes = lax.axis_size("sp") // 4
    blocks = 2 * planes
    side = width // 2
    tiles = width // LANES
    step = max(n for n in (8, 16, 24, 32, 40) if rows % n == 0)
    kept = -(-(span + 2) // 8) * 8
    first, total = slot_table(planes, blocks)
    vmem, dma = pltpu.VMEM, pltpu.SemaphoreType.DMA
    scratch = [
        vmem((rows, width), bf16),
        vmem((rows, width), bf16),
        vmem((span, width), f32),
        vmem((1, width), f32),
        vmem((1, width), f32),
        vmem((4, planes, rows, 2 * block), bf16),
        vmem((planes, side, 2 * block), bf16),
        vmem((tiles, kept, LANES), f32),
        vmem((tiles, rows + 2 * EDGE, LANES), f32),
        vmem((4, EDGE, width), bf16),
        vmem((tiles, rows, LANES), f32),
        vmem((tiles, rows, LANES), f32),
        vmem((4, rows, LANES), f32),
        vmem((4, rows, LANES), f32),
        vmem((4, rows, LANES), f32),
        vmem((5, rows, side), bf16),
        vmem((tiles, rows, LANES), f32),
        vmem((tiles, rows, LANES), f32),
        vmem((2, rows, side), f32),
        vmem((2, 2, rows, side // 2), bf16),
        vmem((2, 2, rows, side // 2), bf16),
        vmem((2, rows, side // 2), bf16),
        vmem((2, rows, side // 2), bf16),
        vmem((blocks, side, block), f32),
        vmem((blocks, side, block), bf16),
        vmem((blocks, side, block), bf16),
        vmem((blocks, side, block), bf16),
        vmem((blocks, side, block), bf16),
        vmem((side, block), bf16),
        vmem((side, block), bf16),
        vmem((side, block), f32),
        vmem((4, side, rows), bf16),
        vmem((tiles, rows + 2 * EDGE, LANES), f32),
        vmem((2, tiles, EDGE, LANES), f32),
        vmem((2, tiles, EDGE, LANES), f32),
        vmem((tiles, kept, LANES), f32),
        vmem((3, tiles // 4, kept, LANES), bf16),
        vmem((planes, tiles // 4, kept, LANES), bf16),
        vmem((tiles // 4, kept, LANES), f32),
        vmem((tiles, kept, LANES), f32),
        vmem((rows, LANES), f32),
        vmem((tiles, kept, LANES), bf16),
        dma((total,)),
        dma((total,)),
        dma((6 + blocks,)),
    ]
    hbm = pl.BlockSpec(memory_space=pl.ANY)
    values = jax.ShapeDtypeStruct((rows, width), bf16)
    given = pl.pallas_call(
        functools.partial(kernel, (rows, width, span, planes, block, step), first),
        out_shape=(
            values,
            values,
            jax.ShapeDtypeStruct((tiles, kept, LANES), f32),
            jax.ShapeDtypeStruct((side, block), f32),
            jax.ShapeDtypeStruct((side, block), bf16),
        ),
        in_specs=[hbm] * 7,
        out_specs=[hbm] * 5,
        scratch_shapes=scratch,
        compiler_params=pltpu.CompilerParams(
            collective_id=0, has_side_effects=True, vmem_limit_bytes=62 * 2**20
        ),
    )(
        value_in,
        gate_in,
        taps,
        norm_gain.reshape(1, width),
        norm_bias.reshape(1, width),
        proj_weight,
        out_grad,
    )
    value_grad, gate_grad, tap_grad, gain_grad, bias_grad, weight_grad = pl.pallas_call(
        functools.partial(write_out, span),
        out_shape=(
            values,
            values,
            jax.ShapeDtypeStruct((span, width), f32),
            jax.ShapeDtypeStruct((1, width), f32),
            jax.ShapeDtypeStruct((1, width), f32),
            jax.ShapeDtypeStruct((width, block), f32),
        ),
        in_specs=[hbm] * 5,
        out_specs=[hbm] * 6,
        scratch_shapes=[
            vmem((rows, width), bf16),
            vmem((rows, width), bf16),
            vmem((tiles, kept, LANES), f32),
            vmem((side, block), f32),
            vmem((side, block), bf16),
            vmem((span, width), f32),
            vmem((1, width), f32),
            vmem((1, width), f32),
            vmem((side, block), f32),
            dma((5,)),
            dma((7,)),
        ],
        compiler_params=pltpu.CompilerParams(vmem_limit_bytes=62 * 2**20),
    )(*given)
    return (
        value_grad,
        gate_grad,
        tap_grad,
        gain_grad.reshape(width),
        bias_grad.reshape(width),
        weight_grad,
    )


def solution(mesh):
    fused = mesh.shape["tp"] == 2 and mesh.shape["sp"] % 4 == 0
    return jax.shard_map(
        fused_on_device if fused else on_device,
        mesh=mesh,
        in_specs=(
            P("sp", "tp"),
            P("sp", "tp"),
            P(None, "tp"),
            P("tp"),
            P("tp"),
            P("tp", "sp"),
            P("sp", None),
        ),
        out_specs=(P("sp", "tp"), P("sp", "tp"), P(None, "tp"), P("tp"), P("tp"), P("tp", "sp")),
        check_vma=False,
    )
```

```python
import functools
import jax
import jax.numpy as jnp
from jax import lax
from jax.experimental import pallas as pl
from jax.experimental.pallas import tpu as pltpu
from jax.sharding import PartitionSpec as P


def padded_rows(cells, width):
    count = lax.axis_size("sp")
    ends = count - 1
    rows = cells.shape[0]
    before = lax.ppermute(cells[rows - width :], "sp", [(i, i + 1) for i in range(ends)])
    after = lax.ppermute(cells[:width], "sp", [(i + 1, i) for i in range(ends)])
    return jnp.concatenate([before, cells, after], axis=0)


def on_device(*arrays):
    return compute(*arrays)


def compute(value_in, gate_in, taps, norm_gain, norm_bias, proj_weight, out_grad):
    f32, bf16 = jnp.float32, jnp.bfloat16
    rows, local_width = value_in.shape
    span = taps.shape[0]
    half = span // 2
    tp = lax.axis_size("tp")
    count = lax.axis_size("sp")
    inner = 1 << ((count.bit_length() - 1) // 2)
    outer = count // inner
    width_all = local_width * tp
    block = proj_weight.shape[1]
    me = lax.axis_index("sp")
    plane, place = me // inner, me % inner
    core = lax.axis_index("tp")

    def swap(array, d):
        return lax.ppermute(
            array, "sp", [(i, i - i % inner + ((i % inner) ^ d)) for i in range(count)]
        )

    def shift(array, e):
        return lax.ppermute(array, "sp", [(i, (i + e * inner) % count) for i in range(count)])

    def across(array, t):
        return lax.ppermute(array, "tp", [(c, c ^ t) for c in range(tp)])

    def tp_sum(array):
        return array + sum(across(array, t) for t in range(1, tp))

    gate_sig = jax.nn.sigmoid(gate_in.astype(f32))
    value_f = value_in.astype(f32)
    mixed = (value_f * gate_sig).astype(bf16)
    padded = padded_rows(mixed, half).astype(f32)

    def columns_of(where, first, blocks):
        return jnp.concatenate(
            [
                lax.dynamic_slice_in_dim(
                    out_grad,
                    (((plane + first + e) % outer) * inner + where) * block,
                    block,
                    axis=1,
                )
                for e in range(blocks)
            ],
            axis=1,
        )

    share = outer // tp
    own_columns = columns_of(place, 0, outer)
    arrived = [swap(columns_of(place ^ d, core * share, share), d) for d in range(1, inner)]
    weights = [proj_weight] + [shift(proj_weight, -e) for e in range(1, outer)]
    weight_cols = jnp.concatenate(weights, axis=1)
    cotangents = [own_columns]
    for got in arrived:
        parts = jnp.stack([got] + [across(got, t) for t in range(1, tp)])
        cotangents.append(
            jnp.concatenate(
                [
                    lax.dynamic_index_in_dim(parts, core ^ j, axis=0, keepdims=False)
                    for j in range(tp)
                ],
                axis=1,
            )
        )

    conv = jnp.zeros((rows, local_width), f32)
    for k in range(span):
        conv = conv + taps[k] * padded[k : k + rows]
    mean = tp_sum(jnp.sum(conv, axis=1)) / width_all
    centred = conv - mean[:, None]
    spread = tp_sum(jnp.sum(centred * centred, axis=1)) / width_all
    inv = lax.rsqrt(spread + 1e-06)
    normed = centred * inv[:, None]
    pre = normed * norm_gain + norm_bias
    sig_pre = jax.nn.sigmoid(pre)
    act = (pre * sig_pre).astype(bf16)
    acts = [act] + [swap(act, d) for d in range(1, inner)]

    partial = [
        lax.dot_general(c, weight_cols, (((1,), (1,)), ((), ())), preferred_element_type=f32)
        for c in cotangents
    ]
    act_grad = partial[0]
    sending = lax.optimization_barrier(([p.astype(bf16) for p in partial[1:]], acts))[0]
    for d in range(1, inner):
        got = swap(sending[d - 1], d)
        act_grad = act_grad + got.astype(f32)

    pre_grad = act_grad * sig_pre * (1.0 + pre * (1.0 - sig_pre))
    normed_grad = pre_grad * norm_gain
    sums = tp_sum(
        jnp.stack([jnp.sum(normed_grad, axis=1), jnp.sum(normed_grad * normed, axis=1)])
    )
    first, second = sums[0], sums[1]
    conv_grad = inv[:, None] * (
        normed_grad - first[:, None] / width_all - normed * second[:, None] / width_all
    )
    extended = lax.optimization_barrier(padded_rows(conv_grad, half))
    tap_local = jnp.stack([jnp.sum(conv_grad * padded[k : k + rows], axis=0) for k in range(span)])
    gain_local = jnp.sum(pre_grad * normed, axis=0)
    bias_local = jnp.sum(pre_grad, axis=0)
    small = jnp.concatenate([tap_local, gain_local[None], bias_local[None]], axis=0)
    small = small + sum(swap(small, d) for d in range(1, inner))
    small = small + sum(shift(small, e) for e in range(1, outer))
    tap_grad, gain_grad, bias_grad = small[:span], small[span], small[span + 1]

    mixed_grad = jnp.zeros((rows, local_width), f32)
    for k in range(span):
        mixed_grad = mixed_grad + taps[k] * extended[2 * half - k : 2 * half - k + rows]
    value_grad = (mixed_grad * gate_sig).astype(bf16)
    gate_grad = (mixed_grad * value_f * gate_sig * (1.0 - gate_sig)).astype(bf16)

    weight_part = lax.dot_general(
        jnp.concatenate(acts, axis=0),
        jnp.concatenate(cotangents, axis=0),
        (((0,), (0,)), ((), ())),
        preferred_element_type=f32,
    )
    weight_grad = weight_part[:, :block]
    for e in range(1, outer):
        sent = weight_part[:, e * block : (e + 1) * block].astype(bf16)
        got = shift(sent, e)
        weight_grad = weight_grad + got.astype(f32)
    return (value_grad, gate_grad, tap_grad, gain_grad, bias_grad, weight_grad)


LANES = 128
EDGE = 16
GROUP = 31
MESH = pl.DeviceIdType.MESH


def slot_table(planes, blocks):
    parts = blocks // 2
    sizes = {
        "halo": 2,
        "cols_x": parts,
        "cols_x_core": parts,
        "cols_d": parts,
        "cols_d_core": parts,
        "cols_y": parts,
        "cols_y_core": parts,
        "w_y": 1,
        "w_up": 2 * (planes - 1),
        "w_down": 2 * (planes - 1),
        "stats": 1,
        "act_x": 1,
        "act_y": 1,
        "act_d": 1,
        "part_x": 4,
        "part_y": 2,
        "up": blocks,
        "down": blocks,
        "w_back": 1,
        "norm": 1,
        "grad_halo": 2,
        "plane_in": 3,
        "across": planes,
        "plane_out": 3,
    }
    first, total = {}, 0
    for name, size in sizes.items():
        first[name] = total
        total += size
    return first, total


def kernel(
    shape,
    first,
    value,
    gate,
    taps_hbm,
    gain_hbm,
    bias_hbm,
    weight,
    cotangent,
    value_grad,
    gate_grad,
    small_grad,
    weight_mine,
    weight_back,
    value_v,
    gate_v,
    taps,
    gain,
    bias,
    cols,
    wh,
    tap_t,
    mixed,
    edge_out,
    edge_in,
    conv,
    dact,
    stat_out,
    stat_in,
    rows_of,
    acts,
    factor_v,
    factor_g,
    part,
    part_out,
    part_in,
    half_out,
    half_in,
    wg,
    up_out,
    down_out,
    up_in,
    down_in,
    back_out,
    back_in,
    weight_v,
    turned,
    grads,
    gedge_out,
    gedge_in,
    small,
    plane_in,
    across,
    owned,
    small_all,
    tile,
    narrow,
    send_sem,
    recv_sem,
    local_sem,
):
    rows, width, span, planes, block, step = shape
    f32, bf16 = jnp.float32, jnp.bfloat16
    blocks = 2 * planes
    parts = blocks // 2
    side = width // 2
    tiles = width // LANES
    tiles_side = tiles // 2
    quarter = tiles // 4
    count = 4 * planes
    half = span // 2
    lead = EDGE - half

    me, core = lax.axis_index("sp"), lax.axis_index("tp")
    z, y, x = lax.div(me, 4), lax.rem(lax.div(me, 2), 2), lax.rem(me, 2)
    yn, xn = 1 - y, 1 - x

    def at(zz, yy, xx):
        return (zz * 4 + yy * 2 + xx, core)

    to_x, to_y, to_d = at(z, y, xn), at(z, yn, x), at(z, yn, xn)
    to_core = (me, 1 - core)
    to_up, to_down = (me + 4, core), (me - 4, core)
    to_next, to_prev = (me + 1, core), (me - 1, core)
    has_up, has_down = z < planes - 1, z > 0
    has_next, has_prev = me < count - 1, me > 0

    pending = []

    def copy(src, dst, name, index, device):
        at_slot = first[name] + index
        return pltpu.make_async_remote_copy(
            src_ref=src,
            dst_ref=dst,
            send_sem=send_sem.at[at_slot],
            recv_sem=recv_sem.at[at_slot],
            device_id=device,
            device_id_type=MESH,
        )

    def send(made, when=None):
        pending.append((made, when))
        if when is None:
            made.start()
        else:
            pl.when(when)(made.start)

    def arrive(made, when=None):
        if when is None:
            made.wait_recv()
        else:
            pl.when(when)(made.wait_recv)

    def lanes(j):
        return pl.ds(pl.multiple_of(j * LANES, LANES), LANES)

    def over(n, body):
        def step_of(j, carry):
            body(j)
            return carry

        lax.fori_loop(0, n, step_of, 0)

    my_rows = pl.ds(pl.multiple_of(y * side, side), side)
    their_rows = pl.ds(pl.multiple_of(yn * side, side), side)

    def column(b):
        return pl.ds(pl.multiple_of(b * block, block), block)

    low = 2 * z < planes
    turn = []
    for q in range(planes - 1):
        down_to = planes - 1 - q
        fall = down_to - jnp.where(down_to <= z, 1, 0)
        rise = q + jnp.where(q >= z, 1, 0)
        turn.append(jnp.where(low, fall, rise))
    turn.append(z)
    mine = [2 * zb + core for zb in turn]

    def cols_at(slab, i):
        return cols.at[slab, lax.div(i, 2), :, column(lax.rem(i, 2))]

    def wh_at(zz, yy):
        return wh.at[zz, :, column(yy)]

    load_v = pltpu.make_async_copy(value, value_v, local_sem.at[0])
    load_g = pltpu.make_async_copy(gate, gate_v, local_sem.at[1])
    load_w = pltpu.make_async_copy(weight.at[my_rows], wh_at(z, y), local_sem.at[2])
    load_c = [
        pltpu.make_async_copy(
            cotangent.at[:, column(2 * i + x)],
            cols.at[0, i // 2, :, (i % 2) * block : (i % 2 + 1) * block],
            local_sem.at[3 + i],
        )
        for i in range(blocks)
    ]
    load_s = [
        pltpu.make_async_copy(src, dst, local_sem.at[3 + blocks + n])
        for n, (src, dst) in enumerate(((taps_hbm, taps), (gain_hbm, gain), (bias_hbm, bias)))
    ]

    barrier = pltpu.get_barrier_semaphore()
    peers = [to_x, to_y, to_d, to_core]
    peers += [at(lax.rem(z + d, planes), y, x) for d in range(1, planes)]
    peers += [(lax.rem(me + 1, count), core), (lax.rem(me + count - 1, count), core)]
    for peer in peers:
        pl.semaphore_signal(barrier, inc=1, device_id=peer, device_id_type=MESH)
    load_v.start()
    load_g.start()
    for made in load_s:
        made.start()

    def w_copies(d, p):
        yb = y if p == 0 else yn
        index = 2 * (d - 1) + p
        below = wh_at(lax.rem(z - d + planes, planes), yb)
        above = wh_at(lax.rem(z + d, planes), yb)
        return (
            copy(below, below, "w_up", index, to_up),
            copy(above, above, "w_down", index, to_down),
        )

    def w_first(p, src, yb):
        dst = wh_at(z, yb)
        send(copy(src, dst, "w_up", p, to_up), has_up)
        send(copy(src, dst, "w_down", p, to_down), has_down)

    def w_forward(d, p):
        up, down = w_copies(d, p)
        yb = y if p == 0 else yn
        below = wh_at(lax.rem(z - d + planes, planes), yb)
        above = wh_at(lax.rem(z + d, planes), yb)
        arrive(up, z >= d)
        if d < planes - 1:
            send(copy(below, below, "w_up", 2 * d + p, to_up), jnp.logical_and(z >= d, has_up))
        arrive(down, z + d < planes)
        if d < planes - 1:
            send(
                copy(above, above, "w_down", 2 * d + p, to_down),
                jnp.logical_and(z + d < planes, has_down),
            )

    w_y = copy(weight.at[their_rows], wh_at(z, y), "w_y", 0, to_y)

    def cols_x(q):
        return copy(
            cotangent.at[:, column(2 * mine[q] + xn)], cols_at(1, mine[q]), "cols_x", q, to_x
        )

    def cols_d(q):
        return copy(cols_at(1, mine[q]), cols_at(3, mine[q]), "cols_d", q, to_y)

    def cols_y(q):
        return copy(
            cotangent.at[:, column(2 * mine[q] + x)], cols_at(2, mine[q]), "cols_y", q, to_y
        )

    def cols_core(slab, name, q):
        ref = cols_at(slab, mine[q])
        return copy(ref, ref, name, q, to_core)

    def pass_x(q):
        arrive(cols_x(q))
        send(cols_d(q))
        send(cols_core(1, "cols_x_core", q))

    def pass_d(q):
        arrive(cols_d(q))
        send(cols_core(3, "cols_d_core", q))

    def pass_y(q):
        arrive(cols_y(q))
        send(cols_core(2, "cols_y_core", q))

    pl.semaphore_wait(barrier, len(peers))
    w_first(0, weight.at[my_rows], y)
    send(w_y)
    send(cols_x(0))
    for made in load_s:
        made.wait()
    load_v.wait()
    load_g.wait()

    def gate_tile(j):
        tap_t[j, 0:span, :] = taps[:, lanes(j)]
        small[j] = jnp.zeros(small.shape[1:], f32)
        sig = jax.nn.sigmoid(gate_v[:, lanes(j)].astype(f32))
        got = (value_v[:, lanes(j)].astype(f32) * sig).astype(bf16).astype(f32)
        mixed[j, EDGE : EDGE + rows, :] = got
        edge_out[0, j] = mixed[j, rows : rows + EDGE, :].astype(bf16)
        edge_out[1, j] = mixed[j, EDGE : 2 * EDGE, :].astype(bf16)

    over(tiles, gate_tile)
    halo = [
        copy(edge_out.at[0], edge_in.at[0], "halo", 0, to_next),
        copy(edge_out.at[1], edge_in.at[1], "halo", 1, to_prev),
    ]
    send(halo[0], has_next)
    send(halo[1], has_prev)
    send(cols_y(0))
    for q in range(1, parts):
        send(cols_x(q))
    load_w.start()
    for made in load_c:
        made.start()

    def fill(made, when, src, dst, at_row):
        @pl.when(when)
        def _():
            made.wait_recv()
            for j in range(tiles):
                dst[j, at_row : at_row + EDGE, :] = src[j].astype(f32)

        @pl.when(jnp.logical_not(when))
        def _():
            for j in range(tiles):
                dst[j, at_row : at_row + EDGE, :] = jnp.zeros((EDGE, LANES), f32)

    def fill_mixed(first_of, when, at_row):
        @pl.when(when)
        def _():
            halo[first_of].wait_recv()
            for j in range(tiles):
                mixed[j, at_row : at_row + EDGE, :] = edge_in[first_of, j].astype(f32)

        @pl.when(jnp.logical_not(when))
        def _():
            for j in range(tiles):
                mixed[j, at_row : at_row + EDGE, :] = jnp.zeros((EDGE, LANES), f32)

    pass_x(0)
    fill_mixed(0, has_prev, 0)
    fill_mixed(1, has_next, EDGE + rows)

    def conv_tile(j):
        for r in range(0, rows, step):
            acc = tap_t[j, 0:1, :] * mixed[j, r + lead : r + lead + step, :]
            for k in range(1, span):
                at_row = r + k + lead
                acc = acc + tap_t[j, k : k + 1, :] * mixed[j, at_row : at_row + step, :]
            conv[j, r : r + step, :] = acc

    over(tiles, conv_tile)
    for r in range(0, rows, step):
        at_rows = slice(r, r + step)
        total = conv[0, at_rows, :]
        for j in range(1, tiles):
            total = total + conv[j, at_rows, :]
        middle = jnp.sum(total, axis=1, keepdims=True) / width
        off = conv[0, at_rows, :] - middle
        square = off * off
        for j in range(1, tiles):
            off = conv[j, at_rows, :] - middle
            square = square + off * off
        stat_out[0, at_rows, :] = total
        stat_out[1, at_rows, :] = square
    stats = copy(stat_out.at[0:2], stat_in.at[0:2], "stats", 0, to_core)
    send(stats)
    arrive(w_y)
    w_first(1, wh_at(z, yn), yn)
    w_forward(1, 0)
    arrive(stats)
    for r in range(0, rows, step):
        at_rows = slice(r, r + step)
        here = jnp.sum(stat_out[0, at_rows, :], axis=1, keepdims=True)
        there = jnp.sum(stat_in[0, at_rows, :], axis=1, keepdims=True)
        both = stat_out[1, at_rows, :] + stat_in[1, at_rows, :]
        apart = (here - there) / width
        spread = jnp.sum(both, axis=1, keepdims=True) / (2 * width) + apart * apart / 4
        inv = lax.rsqrt(spread + 1e-06)
        rows_of[0, at_rows, :] = jnp.broadcast_to((here + there) / (2 * width), (step, LANES))
        rows_of[1, at_rows, :] = jnp.broadcast_to(inv, (step, LANES))

    def act_side(h):
        def act_tile(jj):
            j = h * tiles_side + jj
            normed = (conv[j] - rows_of[0]) * rows_of[1]
            pre = normed * gain[0:1, lanes(j)] + bias[0:1, lanes(j)]
            sig = jax.nn.sigmoid(pre)
            acts[h, :, lanes(jj)] = (pre * sig).astype(bf16)
            conv[j] = normed
            dact[j] = sig * (1.0 + pre * (1.0 - sig))

        over(tiles_side, act_tile)

    act_y = copy(acts.at[yn], acts.at[3], "act_y", 0, to_y)
    act_x = copy(acts.at[y], acts.at[2], "act_x", 0, to_x)
    act_d = copy(acts.at[3], acts.at[4], "act_d", 0, to_x)
    act_side(yn)
    send(act_y)
    act_side(y)
    send(act_x)
    pass_x(1)
    pass_y(0)
    for q in range(2, parts - 1):
        pass_x(q)
    w_forward(1, 1)
    pass_x(parts - 1)
    for q in range(1, parts):
        send(cols_y(q))

    def factor_tile(j):
        sig = jax.nn.sigmoid(gate_v[:, lanes(j)].astype(f32))
        factor_v[j] = sig
        factor_g[j] = value_v[:, lanes(j)].astype(f32) * sig * (1.0 - sig)

    over(tiles, factor_tile)
    turned[0] = acts[y].T
    arrive(act_y)
    send(act_d)
    if planes > 2:
        w_forward(2, 0)
    arrive(act_x)
    turned[1] = acts[2].T
    turned[2] = acts[3].T
    pass_d(0)
    if planes > 2:
        w_forward(2, 1)
    pass_d(1)
    load_w.wait()
    for made in load_c:
        made.wait()

    def weight_of(zb, lo=0, hi=4):
        acc = None
        for slab in range(lo, hi):
            got = jnp.dot(turned[slab], cols[slab, zb], preferred_element_type=f32)
            acc = got if acc is None else acc + got
        for n in range(2):
            got = acc[:, n * block : (n + 1) * block]
            wg[2 * zb + n] = got if lo == 0 else wg[2 * zb + n] + got

    def up_copy(t, p):
        i = 2 * t + (yn if p == 0 else y)
        return copy(up_out.at[i], up_in.at[i], "up", 2 * t + p, to_up)

    def down_copy(t, p):
        i = 2 * t + (yn if p == 0 else y)
        return copy(down_out.at[i], down_in.at[i], "down", 2 * t + p, to_down)

    def fresh(m, p):
        for t, made, out, when in (
            (planes - 1 - m, up_copy(planes - 1 - m, p), up_out, z == 0),
            (m, down_copy(m, p), down_out, z == planes - 1),
        ):
            i = 2 * t + (yn if p == 0 else y)

            @pl.when(when)
            def _():
                out[i] = wg[i].astype(bf16)

            send(made, when)

    def finish(p, among=range(planes)):
        i = 2 * z + (yn if p == 0 else y)
        for t in among:

            @pl.when(z == t)
            def _():
                total = wg[i]
                if t > 0:
                    up_copy(t, p).wait_recv()
                    total = total + up_in[i].astype(f32)
                if t < planes - 1:
                    down_copy(t, p).wait_recv()
                    total = total + down_in[i].astype(f32)
                if p == 0:
                    back_out[...] = total.astype(bf16)
                else:
                    weight_v[...] = total

    back = copy(back_out, back_in, "w_back", 0, to_y)
    inner = jnp.logical_and(has_up, has_down)
    lower = jnp.logical_and(inner, 2 * z < planes)
    upper = jnp.logical_and(inner, 2 * z >= planes)

    def relay(n, going_up, side_of):
        m, p = n // 2, n % 2
        t = planes - 1 - m if going_up else m
        if not 0 <= m < planes - 1:
            return
        i = 2 * t + (yn if p == 0 else y)
        made = up_copy(t, p) if going_up else down_copy(t, p)
        out, got = (up_out, up_in) if going_up else (down_out, down_in)
        when = jnp.logical_and(side_of, z < t if going_up else z > t)

        @pl.when(when)
        def _():
            made.wait_recv()
            out[i] = (wg[i] + got[i].astype(f32)).astype(bf16)

        send(made, when)

    def serve_near(n):
        relay(n, True, lower)
        relay(n, False, upper)

    def serve_far(n):
        relay(n, False, lower)
        relay(n, True, upper)

    arrive(cols_core(1, "cols_x_core", 0))
    arrive(cols_core(3, "cols_d_core", 0))
    arrive(cols_core(2, "cols_y_core", 0))
    weight_of(turn[0], 0, 3)
    arrive(act_d)
    turned[3] = acts[4].T
    weight_of(turn[0], 3, 4)
    fresh(0, 0)
    fresh(0, 1)
    for d in range(3, planes):
        w_forward(d, 0)
    for q in range(2, parts):
        pass_d(q)
    for d in range(3, planes):
        w_forward(d, 1)

    def product(slab, over_zb=range(planes)):
        acc = None
        for zb in over_zb:
            got = lax.dot_general(
                cols[slab, zb], wh[zb], (((1,), (1,)), ((), ())), preferred_element_type=f32
            )
            acc = got if acc is None else acc + got
        return acc

    part_x = [
        [copy(part_out.at[n, h], part_in.at[n, h], "part_x", 2 * n + h, to_x) for h in range(2)]
        for n in range(2)
    ]
    cut = side // 2

    def partial(slab, n):
        got = product(slab)
        for h in range(2):
            part_out[n, h] = got[:, h * cut : (h + 1) * cut].astype(bf16)
            send(part_x[n][h])

    for q in range(1, parts):
        arrive(cols_core(3, "cols_d_core", q))
    partial(3, 1)
    for q in range(1, parts):
        arrive(cols_core(1, "cols_x_core", q))
    partial(1, 0)
    pass_y(1)
    part[0] = product(0)
    arrive(cols_core(2, "cols_y_core", 1))
    weight_of(turn[1])
    fresh(1, 0)
    serve_near(0)
    for q in range(2, parts):
        if q == parts - 1:
            part[1] = product(2, turn[0 : parts - 1])
        pass_y(q)
        arrive(cols_core(2, "cols_y_core", q))
    part[1] = part[1] + product(2, turn[parts - 1 :])
    part_y = [copy(half_out.at[h], half_in.at[h], "part_y", h, to_y) for h in range(2)]

    def fold(h):
        arrive(part_x[1][h])
        got = part[1, :, h * cut : (h + 1) * cut] + part_in[1, h].astype(f32)
        half_out[h] = got.astype(bf16)
        send(part_y[h])

    fold(0)
    for q in range(2, planes - 1):
        weight_of(turn[q])
        fresh(q, 0)
        fresh(q - 1, 1)
    serve_near(1)
    serve_far(0)
    fold(1)
    weight_of(turn[planes - 1])
    stat_out[2] = jnp.zeros((rows, LANES), f32)
    stat_out[3] = jnp.zeros((rows, LANES), f32)

    def back_tile(j, got):
        pre_grad = got * dact[j]
        normed = conv[j]
        scaled = pre_grad * gain[0:1, lanes(j)]
        crossed = pre_grad * normed
        dact[j] = scaled
        stat_out[2] = stat_out[2] + scaled
        stat_out[3] = stat_out[3] + scaled * normed
        small[j, span : span + 1, :] = jnp.sum(crossed, axis=0, keepdims=True)
        small[j, span + 1 : span + 2, :] = jnp.sum(pre_grad, axis=0, keepdims=True)

    tiles_cut = tiles_side // 2

    def back_mine(h):
        arrive(part_x[0][h])

        def one(jj):
            at_side = lanes(h * tiles_cut + jj)
            got = part[0, :, at_side] + part_in[0, h, :, lanes(jj)].astype(f32)
            back_tile(y * tiles_side + h * tiles_cut + jj, got)

        over(tiles_cut, one)

    def back_theirs(h):
        arrive(part_y[h])

        def one(jj):
            back_tile(yn * tiles_side + h * tiles_cut + jj, half_in[h, :, lanes(jj)].astype(f32))

        over(tiles_cut, one)

    back_mine(0)
    serve_near(2)
    back_theirs(0)
    back_mine(1)
    finish(0, sorted({0, planes - 1}))
    send(back, jnp.logical_not(inner))
    back_theirs(1)
    norm = copy(stat_out.at[2:4], stat_in.at[2:4], "norm", 0, to_core)
    send(norm)
    serve_far(1)
    arrive(norm)
    for r in range(0, rows, step):
        at_rows = slice(r, r + step)
        for n in range(2):
            both = stat_out[2 + n, at_rows, :] + stat_in[2 + n, at_rows, :]
            got = jnp.sum(both, axis=1, keepdims=True) / (2 * width)
            rows_of[2 + n, at_rows, :] = jnp.broadcast_to(got, (step, LANES))

    def grad_tile(j):
        grads[j, EDGE : EDGE + rows, :] = rows_of[1] * (
            dact[j] - rows_of[2] - conv[j] * rows_of[3]
        )
        gedge_out[0, j] = grads[j, rows : rows + EDGE, :].astype(bf16)
        gedge_out[1, j] = grads[j, EDGE : 2 * EDGE, :].astype(bf16)

    over(tiles, grad_tile)
    grad_prev = copy(gedge_out.at[0], gedge_in.at[0], "grad_halo", 0, to_next)
    grad_next = copy(gedge_out.at[1], gedge_in.at[1], "grad_halo", 1, to_prev)
    send(grad_prev, has_next)
    send(grad_next, has_prev)

    def tap_tile(j):
        for at in range(0, span, GROUP):
            ks = range(at, min(at + GROUP, span))
            acc = {}
            for r in range(0, rows, step):
                own = grads[j, r + EDGE : r + EDGE + step, :]
                for k in ks:
                    got = own * mixed[j, r + k + lead : r + k + lead + step, :]
                    folded = jnp.sum(got.reshape(step // 8, 8, LANES), axis=0)
                    acc[k] = acc[k] + folded if k in acc else folded
            for k in ks:
                small[j, k : k + 1, :] = jnp.sum(acc[k], axis=0, keepdims=True)

    place = 2 * y + x
    near = [(to_d, 2 * yn + xn), (to_y, 2 * yn + x), (to_x, 2 * y + xn)]
    own_tiles = pl.ds(place * quarter, quarter)
    gather = [
        copy(narrow.at[pl.ds(p * quarter, quarter)], plane_in.at[n], "plane_in", n, dev)
        for n, (dev, p) in enumerate(near)
    ]
    for n, (dev, p) in enumerate(near):
        over(quarter, lambda jj: tap_tile(p * quarter + jj))
        theirs = pl.ds(p * quarter, quarter)
        narrow[theirs] = small[theirs].astype(bf16)
        send(gather[n])
    over(quarter, lambda jj: tap_tile(place * quarter + jj))
    finish(0, range(1, planes - 1))
    send(back, inner)

    def mixed_tile(j):
        for r in range(0, rows, step):
            at_row = r + EDGE + half
            acc = tap_t[j, 0:1, :] * grads[j, at_row : at_row + step, :]
            for k in range(1, span):
                at_row = r + EDGE + half - k
                acc = acc + tap_t[j, k : k + 1, :] * grads[j, at_row : at_row + step, :]
            tile[r : r + step, :] = acc
        got = tile[...]
        value_v[:, lanes(j)] = (got * factor_v[j]).astype(bf16)
        gate_v[:, lanes(j)] = (got * factor_g[j]).astype(bf16)

    def mixed_tiles(lo, hi):
        lax.fori_loop(lo, hi, lambda j, c: (mixed_tile(j), c)[1], 0)

    def across_out():
        for d in range(1, planes):
            arrive(copy(across.at[z], across.at[z], "across", d, to_core))
        total = across[0].astype(f32)
        for d in range(1, planes):
            total = total + across[d].astype(f32)
        owned[...] = total
        small_all[own_tiles] = total
        for made in spread_out:
            send(made)

    spread_out = [
        copy(owned, small_all.at[own_tiles], "plane_out", n, dev) for n, (dev, p) in enumerate(near)
    ]
    for made in gather:
        arrive(made)
    joined = small[own_tiles]
    for n in range(3):
        joined = joined + plane_in[n].astype(f32)
    across[z] = joined.astype(bf16)
    for d in range(1, planes):
        made = copy(across.at[z], across.at[z], "across", d, at(lax.rem(z + d, planes), y, x))
        send(made)
    for n in range(3, 2 * (planes - 1)):
        serve_near(n)
        serve_far(n - 1)
    serve_far(2 * planes - 3)
    for m in range(2, planes - 1):
        fresh(m, 1)
    fill(grad_prev, has_prev, gedge_in.at[0], grads, 0)
    fill(grad_next, has_next, gedge_in.at[1], grads, EDGE + rows)
    mixed_tiles(0, 3 * quarter)
    across_out()
    mixed_tiles(3 * quarter, tiles)
    stores = [
        pltpu.make_async_copy(value_v, value_grad, local_sem.at[0]),
        pltpu.make_async_copy(gate_v, gate_grad, local_sem.at[1]),
        pltpu.make_async_copy(weight_v, weight_mine, local_sem.at[2]),
        pltpu.make_async_copy(small_all, small_grad, local_sem.at[3]),
        pltpu.make_async_copy(back_in, weight_back, local_sem.at[4]),
    ]
    stores[0].start()
    stores[1].start()

    finish(1)
    stores[2].start()
    for made in spread_out:
        arrive(made)
    stores[3].start()
    arrive(back)
    stores[4].start()
    for made, when in pending:
        if when is None:
            made.wait_send()
        else:
            pl.when(when)(made.wait_send)
    for made in stores:
        made.wait()


def write_out(
    span,
    value_in,
    gate_in,
    small_in,
    mine_in,
    back_in,
    value_out,
    gate_out,
    tap_out,
    gain_out,
    bias_out,
    weight_out,
    value_v,
    gate_v,
    small_v,
    mine_v,
    back_v,
    tap_v,
    gain_v,
    bias_v,
    wide_v,
    in_sem,
    out_sem,
):
    side = mine_v.shape[0]
    tiles = small_v.shape[0]
    y = lax.rem(lax.div(lax.axis_index("sp"), 2), 2)

    def rows_at(h):
        return pl.ds(pl.multiple_of(h * side, side), side)

    pairs = (
        (back_in, back_v),
        (small_in, small_v),
        (value_in, value_v),
        (gate_in, gate_v),
        (mine_in, mine_v),
    )
    loads = [pltpu.make_async_copy(a, b, in_sem.at[n]) for n, (a, b) in enumerate(pairs)]
    pairs = (
        (wide_v, weight_out.at[rows_at(1 - y)]),
        (tap_v, tap_out),
        (gain_v, gain_out),
        (bias_v, bias_out),
        (value_v, value_out),
        (gate_v, gate_out),
        (mine_v, weight_out.at[rows_at(y)]),
    )
    stores = [pltpu.make_async_copy(a, b, out_sem.at[n]) for n, (a, b) in enumerate(pairs)]
    for made in loads:
        made.start()
    loads[0].wait()
    wide_v[...] = back_v[...].astype(jnp.float32)
    stores[0].start()
    loads[1].wait()
    for j in range(tiles):
        at_lanes = slice(j * LANES, (j + 1) * LANES)
        tap_v[:, at_lanes] = small_v[j, 0:span, :]
        gain_v[:, at_lanes] = small_v[j, span : span + 1, :]
        bias_v[:, at_lanes] = small_v[j, span + 1 : span + 2, :]
    for n in (1, 2, 3):
        stores[n].start()
    for n in (2, 3, 4):
        loads[n].wait()
        stores[n + 2].start()
    for made in stores:
        made.wait()


def fused_on_device(value_in, gate_in, taps, norm_gain, norm_bias, proj_weight, out_grad):
    f32, bf16 = jnp.float32, jnp.bfloat16
    rows, width = value_in.shape
    span = taps.shape[0]
    block = proj_weight.shape[1]
    planes = lax.axis_size("sp") // 4
    blocks = 2 * planes
    side = width // 2
    tiles = width // LANES
    step = max(n for n in (8, 16, 24, 32, 40) if rows % n == 0)
    kept = -(-(span + 2) // 8) * 8
    first, total = slot_table(planes, blocks)
    vmem, dma = pltpu.VMEM, pltpu.SemaphoreType.DMA
    scratch = [
        vmem((rows, width), bf16),
        vmem((rows, width), bf16),
        vmem((span, width), f32),
        vmem((1, width), f32),
        vmem((1, width), f32),
        vmem((4, planes, rows, 2 * block), bf16),
        vmem((planes, side, 2 * block), bf16),
        vmem((tiles, kept, LANES), f32),
        vmem((tiles, rows + 2 * EDGE, LANES), f32),
        vmem((2, tiles, EDGE, LANES), bf16),
        vmem((2, tiles, EDGE, LANES), bf16),
        vmem((tiles, rows, LANES), f32),
        vmem((tiles, rows, LANES), f32),
        vmem((4, rows, LANES), f32),
        vmem((4, rows, LANES), f32),
        vmem((4, rows, LANES), f32),
        vmem((5, rows, side), bf16),
        vmem((tiles, rows, LANES), f32),
        vmem((tiles, rows, LANES), f32),
        vmem((2, rows, side), f32),
        vmem((2, 2, rows, side // 2), bf16),
        vmem((2, 2, rows, side // 2), bf16),
        vmem((2, rows, side // 2), bf16),
        vmem((2, rows, side // 2), bf16),
        vmem((blocks, side, block), f32),
        vmem((blocks, side, block), bf16),
        vmem((blocks, side, block), bf16),
        vmem((blocks, side, block), bf16),
        vmem((blocks, side, block), bf16),
        vmem((side, block), bf16),
        vmem((side, block), bf16),
        vmem((side, block), f32),
        vmem((4, side, rows), bf16),
        vmem((tiles, rows + 2 * EDGE, LANES), f32),
        vmem((2, tiles, EDGE, LANES), bf16),
        vmem((2, tiles, EDGE, LANES), bf16),
        vmem((tiles, kept, LANES), f32),
        vmem((3, tiles // 4, kept, LANES), bf16),
        vmem((planes, tiles // 4, kept, LANES), bf16),
        vmem((tiles // 4, kept, LANES), f32),
        vmem((tiles, kept, LANES), f32),
        vmem((rows, LANES), f32),
        vmem((tiles, kept, LANES), bf16),
        dma((total,)),
        dma((total,)),
        dma((6 + blocks,)),
    ]
    hbm = pl.BlockSpec(memory_space=pl.ANY)
    values = jax.ShapeDtypeStruct((rows, width), bf16)
    given = pl.pallas_call(
        functools.partial(kernel, (rows, width, span, planes, block, step), first),
        out_shape=(
            values,
            values,
            jax.ShapeDtypeStruct((tiles, kept, LANES), f32),
            jax.ShapeDtypeStruct((side, block), f32),
            jax.ShapeDtypeStruct((side, block), bf16),
        ),
        in_specs=[hbm] * 7,
        out_specs=[hbm] * 5,
        scratch_shapes=scratch,
        compiler_params=pltpu.CompilerParams(
            collective_id=0, has_side_effects=True, vmem_limit_bytes=62 * 2**20
        ),
    )(
        value_in,
        gate_in,
        taps,
        norm_gain.reshape(1, width),
        norm_bias.reshape(1, width),
        proj_weight,
        out_grad,
    )
    value_grad, gate_grad, tap_grad, gain_grad, bias_grad, weight_grad = pl.pallas_call(
        functools.partial(write_out, span),
        out_shape=(
            values,
            values,
            jax.ShapeDtypeStruct((span, width), f32),
            jax.ShapeDtypeStruct((1, width), f32),
            jax.ShapeDtypeStruct((1, width), f32),
            jax.ShapeDtypeStruct((width, block), f32),
        ),
        in_specs=[hbm] * 5,
        out_specs=[hbm] * 6,
        scratch_shapes=[
            vmem((rows, width), bf16),
            vmem((rows, width), bf16),
            vmem((tiles, kept, LANES), f32),
            vmem((side, block), f32),
            vmem((side, block), bf16),
            vmem((span, width), f32),
            vmem((1, width), f32),
            vmem((1, width), f32),
            vmem((side, block), f32),
            dma((5,)),
            dma((7,)),
        ],
        compiler_params=pltpu.CompilerParams(vmem_limit_bytes=62 * 2**20),
    )(*given)
    return (
        value_grad,
        gate_grad,
        tap_grad,
        gain_grad.reshape(width),
        bias_grad.reshape(width),
        weight_grad,
    )


def solution(mesh):
    fused = mesh.shape["tp"] == 2 and mesh.shape["sp"] % 4 == 0
    return jax.shard_map(
        fused_on_device if fused else on_device,
        mesh=mesh,
        in_specs=(
            P("sp", "tp"),
            P("sp", "tp"),
            P(None, "tp"),
            P("tp"),
            P("tp"),
            P("tp", "sp"),
            P("sp", None),
        ),
        out_specs=(P("sp", "tp"), P("sp", "tp"), P(None, "tp"), P("tp"), P("tp"), P("tp", "sp")),
        check_vma=False,
    )
```
